512 devices in a mesh: sp: 64 (over z, y), tp: 8 (over x, core).
Axes of the slice: x: 4, y: 8, z: 8, core: 2. Of those that a mesh axis runs over, the one named last changes fastest.
Arguments:
- tokens: bfloat16 [49152, 2048], P(('sp', 'tp')), may hold values from -6 to 6
- input_norm_gain: bfloat16 [2048], replicated, may hold values from 0.099609375 to 1.8984375
- convolution_outer_weight: bfloat16 [2048, 1024], P(None, 'tp'), may hold values from -0.125 to 0.125
- convolution_inner_weight: bfloat16 [2048, 1024], P(None, 'tp'), may hold values from -0.125 to 0.125
- convolution_signal_weight: bfloat16 [2048, 1024], P(None, 'tp'), may hold values from -0.125 to 0.125
- convolution_kernel_taps: bfloat16 [3, 1024], replicated, may hold values from -3.5 to 3.5
- memory_query_matrix: bfloat16 [2048, 512], P(None, 'tp'), may hold values from -0.125 to 0.125
- memory_key_matrix: bfloat16 [2048, 512], P(None, 'tp'), may hold values from -0.125 to 0.125
- memory_value_matrix: bfloat16 [2048, 1024], P(None, 'tp'), may hold values from -0.125 to 0.125
- output_gate_weight: bfloat16 [2048, 1024], P(None, 'tp'), may hold values from -0.125 to 0.125
- input_gate_weight: bfloat16 [2048, 8], replicated, may hold values from -0.5 to 0.5
- forget_gate_weight: bfloat16 [2048, 8], replicated, may hold values from -0.125 to 0.125
- input_gate_bias: float32 [8], replicated, may hold values from -1 to 125
- forget_gate_bias: float32 [8], replicated, may hold values from 3.5 to 12.5
- position_forget_factor: float32 [49152], P('sp'), may hold values from 0.5 to 2
- extra_log_decay: float32 [49152, 8], P('sp'), may hold values from -0.7 to 0
- starting_memory_state: float32 [8, 64, 128], replicated, may hold values from -6 to 6
- starting_log_scale: float32 [8], replicated, may hold values from 5 to 125
- head_norm_gain: bfloat16 [1024], replicated, may hold values from 0.099609375 to 1.8984375
- convolution_output_weight: bfloat16 [1024, 2048], P('tp'), may hold values from -0.125 to 0.125
- memory_output_weight: bfloat16 [1024, 2048], P('tp'), may hold values from -0.125 to 0.125
Outputs:
- mixed: bfloat16 [49152, 2048], P(('sp', 'tp'))
The draws below stay inside these ranges and needn't reach their ends.
All inputs are finite; a program needn't handle non-finite values.
Results may differ from the reference program's by a relative error of at most 0.035.
Values may be sent and summed in bfloat16 or wider, within the bound.
No kernel may reach another device: no remote copies, remote signals or barrier semaphores. Data moves between devices by JAX's collectives and lax.ppermute only.
A program may use at most 64 MiB of HBM per device.

```python
import jax
import jax.numpy as jnp
from jax import lax

D = 2048
CONV = 1024
WIDTH = 3
MH = 8
DQK = 64
DV = 128
SPAN = 128
TOKENS = 49152
N_TP = 8


def draw_input_gate_bias(key, part):
    return jax.random.uniform(key, (MH,), jnp.float32, -1.0, 1.0)


def draw_forget_gate_bias(key, part):
    order_key = jax.random.fold_in(key, 11)
    level_key = jax.random.fold_in(key, 12)
    ranking = jax.random.permutation(order_key, MH)
    slow_count = MH // 2
    jitter = jax.random.uniform(level_key, (MH,), jnp.float32, 0.0, 1.0)
    return jnp.where(ranking < slow_count, 11.5 + jitter, 3.5 + jitter)


def draw_position_forget_factor(key, part):
    levels = jnp.exp(jax.random.uniform(key, (TOKENS // SPAN,), jnp.float32, jnp.log(0.5), jnp.log(2.0)))
    return jnp.repeat(levels, SPAN)


def draw_extra_log_decay(key, part):
    place_key = jax.random.fold_in(key, 21)
    size_key = jax.random.fold_in(key, 22)
    spots = jax.random.randint(place_key, (2, MH), 0, TOKENS)
    amounts = jnp.log(jax.random.uniform(size_key, (2, MH), jnp.float32, 0.5, 0.8))
    positions = jnp.arange(TOKENS, dtype=jnp.int32)[:, None, None]
    hits = positions == spots[None]
    return jnp.sum(jnp.where(hits, amounts[None], 0.0), axis=1)


def draw_starting_log_scale(key, part):
    return jax.random.uniform(key, (MH,), jnp.float32, 9.0, 12.0)


def shard_levels(own_key, extent, shards, low, top_value):
    factor_of = 1.0
    for position, blocks in shards:
        heights = jax.random.uniform(jax.random.fold_in(jax.random.fold_in(own_key, 6), position), (blocks,), jnp.float32, low / len(shards), top_value / len(shards))
        factor_of = factor_of * jnp.repeat(jnp.exp(heights), extent[position] // blocks).reshape((-1,) + (1,) * (len(extent) - 1 - position))
    return factor_of


def gaussian(stream_key, dims, width, limit, cuts=(), kind=jnp.bfloat16):
    drawn = jax.random.normal(stream_key, dims, jnp.float32) * width
    if len(cuts) > 0:
        drawn = shard_levels(stream_key, dims, cuts, -0.22, 0.18) * drawn
    return jnp.clip(drawn, min=-limit, max=limit).astype(kind)


def setup_inputs(seed: int = 0) -> dict:
    splits = jax.random.split(jax.random.key(seed), 22)
    return {
        "tokens": gaussian(splits[0], (TOKENS, D), 1.0, 6.0, ((0, 512),)),
        "input_norm_gain": jnp.clip(1.0 + 0.18 * jax.random.normal(splits[1], (D,), jnp.float32), 0.099609375, 1.8984375).astype(jnp.bfloat16),
        "convolution_outer_weight": gaussian(splits[2], (D, CONV), D ** -0.5, 0.125, ((1, 8),)),
        "convolution_inner_weight": gaussian(splits[3], (D, CONV), D ** -0.5, 0.125, ((1, 8),)),
        "convolution_signal_weight": gaussian(splits[4], (D, CONV), D ** -0.5, 0.125, ((1, 8),)),
        "convolution_kernel_taps": gaussian(splits[5], (WIDTH, CONV), WIDTH ** -0.5, 3.5),
        "memory_query_matrix": gaussian(splits[6], (D, MH * DQK), D ** -0.5, 0.125, ((1, 8),)),
        "memory_key_matrix": gaussian(splits[7], (D, MH * DQK), D ** -0.5, 0.125, ((1, 8),)),
        "memory_value_matrix": gaussian(splits[8], (D, MH * DV), D ** -0.5, 0.125, ((1, 8),)),
        "output_gate_weight": gaussian(splits[9], (D, MH * DV), D ** -0.5, 0.125, ((1, 8),)),
        "input_gate_weight": gaussian(splits[10], (D, MH), (D // 16) ** -0.5, 0.5),
        "forget_gate_weight": gaussian(splits[11], (D, MH), D ** -0.5, 0.125),
        "input_gate_bias": draw_input_gate_bias(jax.random.fold_in(splits[21], 71), 0),
        "forget_gate_bias": draw_forget_gate_bias(jax.random.fold_in(splits[21], 71), 0),
        "position_forget_factor": draw_position_forget_factor(jax.random.fold_in(splits[21], 71), 0),
        "extra_log_decay": draw_extra_log_decay(jax.random.fold_in(splits[21], 71), 0),
        "starting_memory_state": gaussian(splits[16], (MH, DQK, DV), 1.0, 6.0, (), jnp.float32),
        "starting_log_scale": draw_starting_log_scale(jax.random.fold_in(splits[21], 71), 0),
        "head_norm_gain": jnp.clip(1.0 + 0.18 * jax.random.normal(splits[18], (MH * DV,), jnp.float32), 0.099609375, 1.8984375).astype(jnp.bfloat16),
        "convolution_output_weight": gaussian(splits[19], (CONV, D), (CONV + MH * DV) ** -0.5, 0.125, ((0, 8),)),
        "memory_output_weight": gaussian(splits[20], (MH * DV, D), (CONV + MH * DV) ** -0.5, 0.125, ((0, 8),)),
    }


EPS = 1e-06
HIGHEST_PRECISION = lax.Precision.HIGHEST

def merge_states(earlier, later):
    state_one, peak_one, decay_one = earlier
    state_two, peak_two, decay_two = later
    lifted = peak_one + decay_two
    ceiling = jnp.maximum(lifted, peak_two)
    merged = jnp.exp(lifted - ceiling)[..., None, None] * state_one + jnp.exp(peak_two - ceiling)[..., None, None] * state_two
    return (merged, ceiling, decay_one + decay_two)

def block_terms(key_blocks, value_blocks, input_blocks, forget_blocks):
    cumulative = jnp.cumsum(forget_blocks, axis=2)
    block_total = cumulative[:, :, -1]
    weight_log = block_total[:, :, None] - cumulative + input_blocks
    block_peak = lax.optimization_barrier(jnp.max(weight_log, axis=2))
    weights = jnp.exp(weight_log - block_peak[:, :, None])
    block_state = jnp.einsum('nhld,nhle->nhde', key_blocks * weights[..., None], value_blocks, precision=HIGHEST_PRECISION)
    return (cumulative, block_state, block_peak, block_total)

def block_outputs(query_blocks, key_blocks, value_blocks, input_blocks, cumulative, start_state, start_peak):
    span_len = query_blocks.shape[2]
    carried = cumulative + start_peak[:, :, None]
    pair_log = cumulative[:, :, :, None] - cumulative[:, :, None, :] + input_blocks[:, :, None, :]
    causal = jnp.tril(jnp.ones((span_len, span_len), dtype=bool))
    pair_log = jnp.where(causal, pair_log, -jnp.inf)
    ceiling = jnp.maximum(carried, lax.optimization_barrier(jnp.max(pair_log, axis=3)))
    scores = jnp.einsum('nhtd,nhsd->nhts', query_blocks, key_blocks, precision=HIGHEST_PRECISION) * jnp.exp(pair_log - ceiling[..., None])
    local_part = jnp.einsum('nhts,nhse->nhte', scores, value_blocks, precision=HIGHEST_PRECISION)
    remote = jnp.einsum('nhtd,nhde->nhte', query_blocks, start_state, precision=HIGHEST_PRECISION)
    return jnp.exp(carried - ceiling)[..., None] * remote + local_part

def reference(tokens, input_norm_gain, convolution_outer_weight, convolution_inner_weight, convolution_signal_weight, convolution_kernel_taps, memory_query_matrix, memory_key_matrix, memory_value_matrix, output_gate_weight, input_gate_weight, forget_gate_weight, input_gate_bias, forget_gate_bias, position_forget_factor, extra_log_decay, starting_memory_state, starting_log_scale, head_norm_gain, convolution_output_weight, memory_output_weight):
    row_count = tokens.shape[0]
    widened = tokens.astype(jnp.float32)
    normed = (widened * lax.rsqrt(lax.optimization_barrier(jnp.mean(widened * widened, axis=1, keepdims=True)) + EPS) * input_norm_gain.astype(jnp.float32)).astype(jnp.bfloat16)

    def project(weight):
        return jnp.dot(normed, weight, preferred_element_type=jnp.float32).astype(jnp.bfloat16)
    outer_gate = project(convolution_outer_weight)
    inner_gate = project(convolution_inner_weight)
    signal = project(convolution_signal_weight)
    mixed_in = inner_gate.astype(jnp.float32) * signal.astype(jnp.float32)
    tap_count = convolution_kernel_taps.shape[0]
    padded = jnp.pad(mixed_in, ((tap_count - 1, 0), (0, 0)))
    conv_sum = jnp.zeros((row_count, CONV), jnp.float32)
    for offset in range(tap_count):
        conv_sum = conv_sum + convolution_kernel_taps[offset].astype(jnp.float32) * padded[offset:offset + row_count]
    conv_out = (outer_gate.astype(jnp.float32) * conv_sum).astype(jnp.bfloat16)
    queries = project(memory_query_matrix)
    key_rows = project(memory_key_matrix)
    value_rows = project(memory_value_matrix)
    out_gate = project(output_gate_weight)
    log_input = jnp.dot(normed, input_gate_weight, preferred_element_type=jnp.float32) + input_gate_bias
    forget_preactivation = jnp.dot(normed, forget_gate_weight, preferred_element_type=jnp.float32) + forget_gate_bias
    forget_log_values = position_forget_factor[:, None] * jax.nn.log_sigmoid(forget_preactivation) + extra_log_decay
    block_count = row_count // SPAN

    def heads_first(source, column_width):
        return source.astype(jnp.float32).reshape(block_count, SPAN, MH, column_width).transpose(0, 2, 1, 3)

    def gates_first(source):
        return source.reshape(block_count, SPAN, MH).transpose(0, 2, 1)
    query_blocks = heads_first(queries, DQK) * DQK ** (-0.5)
    key_blocks = heads_first(key_rows, DQK)
    value_blocks = heads_first(value_rows, DV)
    input_blocks = gates_first(log_input)
    forget_blocks = gates_first(forget_log_values)
    cumulative, block_state, block_peak, block_total = block_terms(key_blocks, value_blocks, input_blocks, forget_blocks)

    def advance(carried_state, block_item):
        return (merge_states(carried_state, block_item), carried_state[:2])
    start_tuple = (starting_memory_state, starting_log_scale, jnp.zeros((MH,), jnp.float32))
    final_state, starts = lax.scan(advance, start_tuple, (block_state, block_peak, block_total))
    numerator = block_outputs(query_blocks, key_blocks, value_blocks, input_blocks, cumulative, starts[0], starts[1])
    numerator = numerator.transpose(0, 2, 1, 3).reshape(row_count, MH, DV)
    normal_rows = numerator * lax.rsqrt(lax.optimization_barrier(jnp.mean(numerator * numerator, axis=2, keepdims=True)) + EPS)
    memory_out = (normal_rows.reshape(row_count, MH * DV) * head_norm_gain.astype(jnp.float32) * jax.nn.sigmoid(out_gate.astype(jnp.float32))).astype(jnp.bfloat16)
    conv_width = CONV // N_TP
    memory_width = MH * DV // N_TP
    summed = jnp.zeros((row_count, D), jnp.float32)
    for group_index in range(N_TP):
        conv_lo = group_index * conv_width
        memory_lo = group_index * memory_width
        group_term = jnp.dot(conv_out[:, conv_lo:conv_lo + conv_width], convolution_output_weight[conv_lo:conv_lo + conv_width], preferred_element_type=jnp.float32) + jnp.dot(memory_out[:, memory_lo:memory_lo + memory_width], memory_output_weight[memory_lo:memory_lo + memory_width], preferred_element_type=jnp.float32)
        summed = summed + lax.optimization_barrier(group_term.astype(jnp.bfloat16)).astype(jnp.float32)
    return summed.astype(jnp.bfloat16)
```

```python
import functools

import jax
import jax.numpy as jnp
from jax import lax
from jax.experimental import pallas as pl
from jax.experimental.pallas import tpu as pltpu
from jax.sharding import PartitionSpec as P


DQK = 64
DV = 128
EPS = 1e-06
FLOOR = -1e30
F32 = jnp.float32
BF16 = jnp.bfloat16
PAYLOAD = 80

VMEM = pl.BlockSpec(memory_space=pltpu.VMEM)
SMEM = pl.BlockSpec(memory_space=pltpu.SMEM)


def call(body, outs, ins, scratch=(), flops=10**8, limit=48 << 20):
    return pl.pallas_call(
        body,
        out_shape=outs,
        in_specs=ins,
        out_specs=jax.tree.map(lambda _: VMEM, outs),
        scratch_shapes=list(scratch),
        compiler_params=pltpu.CompilerParams(vmem_limit_bytes=limit),
        cost_estimate=pl.CostEstimate(flops=flops, bytes_accessed=1 << 20, transcendentals=0),
    )


def dot(a, b, dims=((1,), (0,))):
    return lax.dot_general(a, b, (dims, ((), ())), preferred_element_type=F32)


def norm_body(tokens, gain, out):
    wide = tokens[...].astype(F32)
    scale = lax.rsqrt(jnp.mean(wide * wide, axis=1, keepdims=True) + EPS)
    out[...] = (wide * scale * gain[...].astype(F32)).astype(BF16)


def fill_rows(place, blocks, rows):
    for i, block in enumerate(blocks):
        start = pl.multiple_of(place[i] * 96, 32)
        rows[pl.ds(start, 96), :] = block[...]


def split3(value):
    high = value.astype(BF16).astype(F32)
    rest = value - high
    middle = rest.astype(BF16).astype(F32)
    return [high, middle, rest - middle]


def lane_scan(value, op, neutral):
    lane = lax.broadcasted_iota(jnp.int32, value.shape, 1)
    step = 1
    while step < 128:
        value = op(value, jnp.where(lane >= step, pltpu.roll(value, step, 1), neutral))
        step *= 2
    return value


def row_scan(value, op, neutral):
    last = jnp.broadcast_to(value[:, 127:128], value.shape)
    row = lax.broadcasted_iota(jnp.int32, value.shape, 0)
    before = jnp.where(row >= 1, pltpu.roll(last, 1, 0), neutral)
    for step in (1, 2, 4):
        before = op(before, jnp.where(row >= step, pltpu.roll(before, step, 0), neutral))
    return before


def rows_of(wide_row):
    pieces = [wide_row[:, 128 * b : 128 * (b + 1)] for b in range(6)]
    return jnp.concatenate(pieces + [jnp.zeros((2, 128), F32)], axis=0)


def state_body(
    place, index, in_bias, forget_bias, b0, b1, b2, b3, b4, b5, b6, b7,
    w_state, w_gate, w_rim, factor, extra, payload, kqv_out, gate_out, rows,
):
    fill_rows(place, (b0, b1, b2, b3, b4, b5, b6, b7), rows)
    head = index[0]
    gates = dot(rows[...], w_gate[...])
    turned = [jnp.transpose(gates[128 * b : 128 * (b + 1), :]) for b in range(6)]
    blank = jnp.zeros((2, 128), F32)
    log_input = jnp.concatenate([t[0:1] for t in turned] + [blank], axis=0) + in_bias[head]
    forget = jnp.concatenate([t[1:2] for t in turned] + [blank], axis=0) + forget_bias[head]
    log_sig = jnp.minimum(forget, 0.0) - jnp.log1p(jnp.exp(-jnp.abs(forget)))
    log_forget = rows_of(factor[...]) * log_sig + rows_of(extra[pl.ds(head, 1), :])
    real = lax.broadcasted_iota(jnp.int32, (8, 128), 0) < 6
    cumul = lane_scan(jnp.where(real, log_forget, 0.0), jnp.add, 0.0)
    cumul = cumul + row_scan(cumul, jnp.add, 0.0)
    level = jnp.where(real, log_input - cumul, FLOOR)
    top = lane_scan(level, jnp.maximum, FLOOR)
    top = jnp.maximum(top, row_scan(top, jnp.maximum, FLOOR))
    total = cumul[5:6, 127:128]
    highest = top[5:6, 127:128]
    peak = jnp.broadcast_to(total + highest, (1, 128))
    weight = jnp.exp(level - highest)
    fill = jnp.zeros((112, 128), F32)
    columns = jnp.transpose(jnp.concatenate([weight, top, fill], axis=0))
    kqv = dot(rows[...], w_state[...]).astype(BF16)
    kqv_out[...] = kqv
    pieces = []
    for b in range(6):
        keys = kqv[128 * b : 128 * (b + 1), 0:DQK].astype(F32)
        pieces.append((keys * columns[:, b : b + 1]).astype(BF16))
    state = dot(jnp.concatenate(pieces, axis=0), kqv[:, 128:256], ((0,), (0,)))
    rim = dot(rows[752:768, :], w_rim[...])
    payload[...] = jnp.concatenate(
        [state]
        + split3(peak)
        + split3(jnp.broadcast_to(total, (1, 128)))
        + [rim[14:16, 0:128], rim[14:16, 128:256], jnp.zeros((PAYLOAD - 74, 128), F32)],
        axis=0,
    ).astype(BF16)
    gate_out[0:8, :] = level
    gate_out[8:136, :] = columns


def local_body(
    place, index, b0, b1, b2, b3, b4, b5, b6, b7, w_rest, taps, kqv, gates,
    local_out, gate_out, conv_out, edge_out, rows,
):
    fill_rows(place, (b0, b1, b2, b3, b4, b5, b6, b7), rows)
    level = gates[0:8, :]
    row = lax.broadcasted_iota(jnp.int32, (128, 128), 0)
    column = lax.broadcasted_iota(jnp.int32, (128, 128), 1)
    causal = row >= column
    for b in range(6):
        high = 128 * (b + 1)
        query = (kqv[128 * b : high, DQK : 2 * DQK].astype(F32) * DQK**-0.5).astype(BF16)
        top = gates[8:136, 8 + b : 9 + b]
        scores = dot(query, kqv[0:high, 0:DQK], ((1,), (1,)))
        parts = []
        for u in range(b + 1):
            power = level[u : u + 1, :] - top
            if u == b:
                power = jnp.where(causal, power, FLOOR)
            parts.append((scores[:, 128 * u : 128 * (u + 1)] * jnp.exp(power)).astype(BF16))
        weights = parts[0] if b == 0 else jnp.concatenate(parts, axis=1)
        local_out[128 * b : high, :] = dot(weights, kqv[0:high, 128:256])
    x = rows[...]
    first = dot(x, w_rest[:, 0:256])
    outer = first[:, 0:128].astype(BF16).astype(F32)
    inner = first[:, 128:256].astype(BF16).astype(F32)
    second = dot(x, w_rest[:, 256:512])
    signal = second[:, 0:128].astype(BF16).astype(F32)
    gate_out[...] = jax.nn.sigmoid(second[:, 128:256].astype(BF16).astype(F32)).astype(BF16)
    head = index[0]
    tap = taps[:, pl.ds(pl.multiple_of(head * 128, 128), 128)].astype(F32)
    mixed = inner * signal
    at = lax.broadcasted_iota(jnp.int32, mixed.shape, 0)
    one = jnp.where(at >= 1, pltpu.roll(mixed, 1, 0), 0.0)
    two = jnp.where(at >= 2, pltpu.roll(mixed, 2, 0), 0.0)
    summed = tap[0:1] * two + tap[1:2] * one + tap[2:3] * mixed
    conv_out[...] = (outer * summed).astype(BF16)
    edge_out[0:16, :] = summed[0:16]
    edge_out[16:32, :] = outer[0:16]


def merged(states, peaks, decays, allowed, upto):
    scales = []
    after = jnp.zeros((1, 128), F32)
    for i in reversed(range(8)):
        scales.append(jnp.where(allowed[i], peaks[i] + after, FLOOR))
        after = after + jnp.where(upto[i], decays[i], 0.0)
    scales = scales[::-1]
    ceiling = functools.reduce(jnp.maximum, scales)
    total = jnp.zeros((DQK, DV), F32)
    for i in range(8):
        factor = jnp.where(allowed[i], jnp.exp(scales[i] - ceiling), 0.0)
        total = total + factor * states[i]
    return total, ceiling, after


def unpack(received):
    wide = [received[i].astype(F32) for i in range(8)]
    return (
        [w[0:64] for w in wide],
        [w[64:65] + w[65:66] + w[66:67] for w in wide],
        [w[67:68] + w[68:69] + w[69:70] for w in wide],
        [w[70:74] for w in wide],
    )


def line_body(index, received, payload, before):
    me = index[1]
    states, peaks, decays, rims = unpack(received)
    every = [True] * 8
    state, peak, decay = merged(states, peaks, decays, every, every)
    payload[...] = jnp.concatenate(
        [state] + split3(peak) + split3(decay) + [rims[7], jnp.zeros((PAYLOAD - 74, 128), F32)],
        axis=0,
    ).astype(BF16)
    earlier = [i < me for i in range(8)]
    state, peak, decay = merged(states, peaks, decays, earlier, earlier)
    rim = jnp.zeros((4, 128), F32)
    for i in range(7):
        rim = jnp.where(me == i + 1, rims[i], rim)
    before[0:64, :] = state
    before[64:72, :] = jnp.concatenate([peak, decay, rim, jnp.zeros((2, 128), F32)], axis=0)


def final_body(
    index, start_scale, received, before, start_state, local, gates, out_gate, kqv, conv,
    edge, taps, gain, out,
):
    head, y, z = index[0], index[1], index[2]
    states, peaks, decays, rims = unpack(received)
    earlier = [i < z for i in range(8)]
    state, peak, decay = merged(states, peaks, decays, earlier, earlier)
    lifted = start_scale[head] + decay
    ceiling = jnp.maximum(lifted, peak)
    state = jnp.exp(lifted - ceiling) * start_state[head] + jnp.exp(peak - ceiling) * state
    lifted = ceiling + before[65:66, :]
    peak = before[64:65, :]
    ceiling = jnp.maximum(lifted, peak)
    state = jnp.exp(lifted - ceiling) * state + jnp.exp(peak - ceiling) * before[0:64, :]
    state = (state * DQK**-0.5).astype(BF16)
    top = gates[8:136, :]
    best = jnp.maximum(top, ceiling)
    keep = jnp.exp(top - best)
    bring = jnp.exp(ceiling - best)
    scale = gain[:, pl.ds(pl.multiple_of(head * 128, 128), 128)].astype(F32)
    for b in range(6):
        here = slice(128 * b, 128 * (b + 1))
        remote = dot(kqv[here, DQK : 2 * DQK], state)
        number = bring[:, 8 + b : 9 + b] * remote + keep[:, 8 + b : 9 + b] * local[here, :]
        spread = lax.rsqrt(jnp.mean(number * number, axis=1, keepdims=True) + EPS)
        out[here, 128:256] = (number * spread * scale * out_gate[here, :].astype(F32)).astype(BF16)
    out[:, 0:128] = conv[...]
    rim = before[66:70, :]
    for i in range(7):
        rim = jnp.where(jnp.logical_and(y == 0, z == i + 1), rims[i], rim)
    past = rim[0:2] * rim[2:4]
    tap = taps[:, pl.ds(pl.multiple_of(head * 128, 128), 128)].astype(F32)
    extra = jnp.concatenate(
        [tap[0:1] * past[0:1] + tap[1:2] * past[1:2], tap[0:1] * past[1:2], jnp.zeros((14, 128), F32)],
        axis=0,
    )
    out[0:16, 0:128] = (edge[16:32, :] * (edge[0:16, :] + extra)).astype(BF16)


def project_body(core, mine, theirs, w_mine, w_theirs, out):
    for x in range(4):
        row = pl.multiple_of(x * 192 + core[0] * 96, 32)
        here = mine[pl.ds(row, 96), :]
        there = theirs[96 * x : 96 * (x + 1), :]
        for n in range(4):
            cut = slice(512 * n, 512 * (n + 1))
            out[x, :, cut] = (dot(here, w_mine[:, cut]) + dot(there, w_theirs[:, cut])).astype(BF16)


def add_body(parts, out):
    total = parts[0].astype(F32)
    for x in range(1, 4):
        total = total + parts[x].astype(F32)
    out[...] = total.astype(BF16)


def tp_moves(move):
    moves = []
    for i in range(8):
        x, core = move(i // 2, i % 2)
        moves.append((i, (x % 4) * 2 + core))
    return moves


UP = tp_moves(lambda x, c: (x + 1, c))
DOWN = tp_moves(lambda x, c: (x - 1, c))
ACROSS = tp_moves(lambda x, c: (x + 2, c))
SWAP = tp_moves(lambda x, c: (x, 1 - c))
X_GROUPS = [[0, 2, 4, 6], [1, 3, 5, 7]]
Y_GROUPS = [[z * 8 + y for y in range(8)] for z in range(8)]
Z_GROUPS = [[z * 8 + y for z in range(8)] for y in range(8)]


def move(value, pairs):
    return lax.ppermute(value, "tp", pairs)


def to_all(value, groups):
    copies = jnp.broadcast_to(value[None], (8, *value.shape))
    return lax.all_to_all(copies, "sp", 0, 0, axis_index_groups=groups)


def on_device(
    tokens, input_norm_gain, w_outer, w_inner, w_signal, taps, w_query, w_key, w_value, w_gate,
    w_input, w_forget, in_bias, forget_bias, factor, extra, start_state, start_scale, head_gain,
    w_conv_out, w_memory_out,
):
    sds = jax.ShapeDtypeStruct
    tp = lax.axis_index("tp")
    sp = lax.axis_index("sp")
    x, core = tp // 2, tp % 2
    index = jnp.stack([tp, sp % 8, sp // 8, core]).astype(jnp.int32)

    normed = call(norm_body, sds((96, 2048), BF16), [VMEM, VMEM])(
        tokens, input_norm_gain.reshape(1, 2048)
    )
    far = move(normed, ACROSS)
    low = move(normed, UP)
    high = move(normed, DOWN)
    twin = move(normed, SWAP)
    sides = move(jnp.concatenate([low, high], axis=0), SWAP)
    far_twin = move(far, SWAP)
    blocks = (normed, low, high, far, twin, sides[0:96], sides[96:192], far_twin)
    place = []
    for swapped in (0, 1):
        for shift in (0, 3, 1, 2):
            place.append(((x + shift) % 4) * 2 + (1 - core if swapped else core))
    place = jnp.stack(place).astype(jnp.int32)

    w_state = jnp.concatenate([w_key, w_query, w_value], axis=1)
    pick = lambda w: lax.dynamic_slice_in_dim(w, tp, 1, 1)
    w_gates = jnp.concatenate(
        [pick(w_input), pick(w_forget), jnp.zeros((2048, 126), BF16)], axis=1
    )
    w_rim = jnp.concatenate([w_inner, w_signal], axis=1)
    w_rest = jnp.concatenate([w_outer, w_inner, w_signal, w_gate], axis=1)

    rows = [pltpu.VMEM((768, 2048), BF16)]
    payload, kqv, gates = call(
        state_body,
        (sds((PAYLOAD, 128), BF16), sds((768, 256), BF16), sds((136, 128), F32)),
        [SMEM] * 4 + [VMEM] * 13,
        rows,
    )(
        place, index, in_bias, forget_bias, *blocks, w_state, w_gates, w_rim,
        factor.reshape(1, 768), extra.T,
    )
    received = to_all(payload, Y_GROUPS)
    local, out_gate, conv, edge = call(
        local_body,
        (sds((768, 128), F32), sds((768, 128), BF16), sds((768, 128), BF16), sds((32, 128), F32)),
        [SMEM] * 2 + [VMEM] * 12,
        rows,
        flops=10**9,
    )(place, index, *blocks, w_rest, taps, kqv, gates)
    payload, before = call(
        line_body, (sds((PAYLOAD, 128), BF16), sds((72, 128), F32)), [SMEM, VMEM]
    )(index, received)
    received = to_all(payload, Z_GROUPS)
    both = call(final_body, sds((768, 256), BF16), [SMEM] * 2 + [VMEM] * 11)(
        index, start_scale, received, before, start_state, local, gates, out_gate, kqv, conv,
        edge, taps, head_gain.reshape(1, 1024),
    )
    w_mine = jnp.concatenate([w_conv_out, w_memory_out], axis=0)
    w_theirs = move(w_mine, SWAP)
    halves = both.reshape(4, 2, 96, 256)
    sent = lax.dynamic_index_in_dim(halves, 1 - core, 1, keepdims=False).reshape(384, 256)
    theirs = move(sent, SWAP)
    terms = call(project_body, sds((4, 96, 2048), BF16), [SMEM] + [VMEM] * 4)(
        index[3:4], both, theirs, w_mine, w_theirs
    )
    parts = lax.all_to_all(terms, "tp", 0, 0, axis_index_groups=X_GROUPS)
    return call(add_body, sds((96, 2048), BF16), [VMEM])(parts)


def solution(mesh):
    in_specs = (
        P(("sp", "tp"), None),
        P(),
        P(None, "tp"),
        P(None, "tp"),
        P(None, "tp"),
        P(),
        P(None, "tp"),
        P(None, "tp"),
        P(None, "tp"),
        P(None, "tp"),
        P(),
        P(),
        P(),
        P(),
        P("sp"),
        P("sp", None),
        P(),
        P(),
        P(),
        P("tp", None),
        P("tp", None),
    )
    return jax.shard_map(
        on_device,
        mesh=mesh,
        in_specs=in_specs,
        out_specs=P(("sp", "tp"), None),
        check_vma=False,
    )
```

```python
import functools

import jax
import jax.numpy as jnp
from jax import lax
from jax.experimental import pallas as pl
from jax.experimental.pallas import tpu as pltpu
from jax.sharding import PartitionSpec as P


DQK = 64
DV = 128
EPS = 1e-06
FLOOR = -1e30
F32 = jnp.float32
BF16 = jnp.bfloat16
PAYLOAD = 80

SPACES = {
    "vmem": (pltpu.VMEM, pltpu.VMEM),
    "hbm": (pltpu.HBM, pltpu.HBM),
    "load": (pltpu.HBM, pltpu.VMEM),
    "smem": (pltpu.HBM, pltpu.SMEM),
}


def call(body, outs, ins, scratch=(), flops=10**8, limit=16 << 20):
    results = pl.pallas_call(
        body,
        out_shape=tuple(SPACES[how][0](shape, kind) for how, shape, kind in outs),
        in_specs=[pl.BlockSpec(memory_space=SPACES[how][1]) for how, _ in ins],
        out_specs=tuple(pl.BlockSpec(memory_space=SPACES[how][1]) for how, _, _ in outs),
        scratch_shapes=list(scratch),
        compiler_params=pltpu.CompilerParams(vmem_limit_bytes=limit),
        cost_estimate=pl.CostEstimate(flops=flops, bytes_accessed=1 << 20, transcendentals=0),
    )(*[pltpu.with_memory_space_constraint(array, SPACES[how][0]) for how, array in ins])
    return results[0] if len(outs) == 1 else results


def tag(how, *arrays):
    return [(how, array) for array in arrays]


def dot(a, b, dims=((1,), (0,))):
    return lax.dot_general(a, b, (dims, ((), ())), preferred_element_type=F32)


def norm_body(tokens, gain, out):
    wide = tokens[...].astype(F32)
    scale = lax.rsqrt(jnp.mean(wide * wide, axis=1, keepdims=True) + EPS)
    out[...] = (wide * scale * gain[...].astype(F32).reshape(1, 2048)).astype(BF16)


def own_tp():
    return lax.axis_index("tp").astype(jnp.int32)


def own_sp():
    return lax.axis_index("sp").astype(jnp.int32)


def places(tp):
    x, core = tp // 2, tp % 2
    return [
        ((x + shift) % 4) * 2 + (1 - core if swapped else core)
        for swapped in (0, 1)
        for shift in (0, 3, 1, 2)
    ]


def stack_body(b0, b1, b2, out):
    out[0:96, :] = b0[...]
    out[96:192, :] = b1[...]
    out[192:288, :] = b2[...]


def split3(value):
    high = value.astype(BF16).astype(F32)
    rest = value - high
    middle = rest.astype(BF16).astype(F32)
    return [high, middle, rest - middle]


def lane_scan(value, op, neutral):
    lane = lax.broadcasted_iota(jnp.int32, value.shape, 1)
    step = 1
    while step < 128:
        value = op(value, jnp.where(lane >= step, pltpu.roll(value, step, 1), neutral))
        step *= 2
    return value


def row_scan(value, op, neutral):
    last = jnp.broadcast_to(value[:, 127:128], value.shape)
    row = lax.broadcasted_iota(jnp.int32, value.shape, 0)
    before = jnp.where(row >= 1, pltpu.roll(last, 1, 0), neutral)
    for step in (1, 2, 4):
        before = op(before, jnp.where(row >= step, pltpu.roll(before, step, 0), neutral))
    return before


def rows_of(wide_row):
    pieces = [wide_row[:, 128 * b : 128 * (b + 1)] for b in range(6)]
    return jnp.concatenate(pieces + [jnp.zeros((2, 128), F32)], axis=0)


def prepare_body(
    in_bias, forget_bias, start_scale, normed, w_key, w_query, w_input, w_forget, w_value,
    w_inner, w_signal, w_conv, w_memory, factor, extra, taps, gain,
    w_turned, w_value_out, w_rim, w_out, aside, sems,
):
    loads = [
        (w_key, w_turned.at[0:64, :]),
        (w_query, w_turned.at[64:128, :]),
        (w_input, w_turned.at[128:136, :]),
        (w_forget, w_turned.at[136:144, :]),
        (w_value, w_value_out),
        (w_inner, w_rim.at[:, 0:128]),
        (w_signal, w_rim.at[:, 128:256]),
        (w_conv, w_out.at[0:128, :]),
        (w_memory, w_out.at[128:256, :]),
    ]
    loads = [pltpu.make_async_copy(a, b, sems.at[i]) for i, (a, b) in enumerate(loads)]
    for load in loads:
        load.start()
    head = own_tp()
    w_turned[144:256, :] = jnp.zeros((112, 2048), BF16)
    aside[0:8, :] = rows_of(factor[...].reshape(1, 768))
    aside[8:16, :] = rows_of(extra[pl.ds(head, 1), :])
    aside[16:24, :] = jnp.full((8, 128), in_bias[head], F32)
    aside[24:32, :] = jnp.full((8, 128), forget_bias[head], F32)
    aside[32:40, :] = jnp.full((8, 128), start_scale[head], F32)
    lanes = pl.ds(pl.multiple_of(head * 128, 128), 128)
    gains = gain[...].astype(F32).reshape(1, 1024)
    own_gain = jnp.zeros((1, 128), F32)
    for i in range(8):
        own_gain = jnp.where(head == i, gains[:, 128 * i : 128 * (i + 1)], own_gain)
    aside[40:48, :] = jnp.concatenate(
        [taps[:, lanes].astype(F32), own_gain, jnp.zeros((4, 128), F32)], axis=0
    )
    for load in loads:
        load.wait()


def state_body(
    b0, b1, b2, b3, twins, b7, w_turned, w_value, w_rim, aside,
    payload, kqv_out, level_out, rows_out, rows, kqv, level_keep, sems,
):
    head = own_tp()
    blocks = [b0, b1, b2, b3] + [twins.at[pl.ds(96 * i, 96), :] for i in range(3)] + [b7]
    for place, block in zip(places(head), blocks):
        rows[pl.ds(pl.multiple_of(place * 96, 32), 96), :] = block[...]
    savings = [
        pltpu.make_async_copy(rows, rows_out, sems.at[0]),
        pltpu.make_async_copy(kqv, kqv_out, sems.at[1]),
        pltpu.make_async_copy(level_keep, level_out, sems.at[2]),
    ]
    savings[0].start()
    first = dot(rows[...], w_turned[...], ((1,), (1,)))
    turned = [jnp.transpose(first[128 * b : 128 * (b + 1), 128:256]) for b in range(6)]
    mine = lax.broadcasted_iota(jnp.int32, (8, 128), 0) == head
    pick = lambda part: jnp.sum(jnp.where(mine, part, 0.0), axis=0, keepdims=True)
    blank = jnp.zeros((2, 128), F32)
    log_input = jnp.concatenate([pick(t[0:8]) for t in turned] + [blank], axis=0) + aside[16:24, :]
    forget = jnp.concatenate([pick(t[8:16]) for t in turned] + [blank], axis=0) + aside[24:32, :]
    log_sig = jnp.minimum(forget, 0.0) - jnp.log1p(jnp.exp(-jnp.abs(forget)))
    log_forget = aside[0:8, :] * log_sig + aside[8:16, :]
    real = lax.broadcasted_iota(jnp.int32, (8, 128), 0) < 6
    until = lax.broadcasted_iota(jnp.int32, (128, 128), 0)
    until = (until <= lax.broadcasted_iota(jnp.int32, (128, 128), 1)).astype(F32)
    cumul = lax.dot_general(
        jnp.where(real, log_forget, 0.0),
        until,
        (((1,), (0,)), ((), ())),
        precision=lax.Precision.HIGHEST,
        preferred_element_type=F32,
    )
    cumul = cumul + row_scan(cumul, jnp.add, 0.0)
    level = jnp.where(real, log_input - cumul, FLOOR)
    total = cumul[5:6, 127:128]
    highest = jnp.max(level, keepdims=True)
    peak = jnp.broadcast_to(total + highest, (1, 128))
    weight = jnp.exp(level - highest)
    columns = jnp.transpose(jnp.concatenate([weight, jnp.zeros((120, 128), F32)], axis=0))
    values = dot(rows[...], w_value[...]).astype(BF16)
    kqv[:, 0:128] = first[:, 0:128].astype(BF16)
    kqv[:, 128:256] = values
    savings[1].start()
    level_keep[...] = level
    savings[2].start()
    pieces = []
    for b in range(6):
        keys = first[128 * b : 128 * (b + 1), 0:DQK].astype(BF16).astype(F32)
        pieces.append((keys * columns[:, b : b + 1]).astype(BF16))
    state = dot(jnp.concatenate(pieces, axis=0), values, ((0,), (0,)))
    rim = dot(rows[752:768, :], w_rim[...])
    packed = jnp.concatenate(
        [state]
        + split3(peak)
        + split3(jnp.broadcast_to(total, (1, 128)))
        + [rim[14:16, 0:128], rim[14:16, 128:256], jnp.zeros((PAYLOAD - 74, 128), F32)],
        axis=0,
    ).astype(BF16)
    for i in range(8):
        payload[i] = packed
    for saving in savings:
        saving.wait()


def local_body(level_in, kqv, local_out, top_out):
    level = level_in[...]
    top = lane_scan(level, jnp.maximum, FLOOR)
    top = jnp.maximum(top, row_scan(top, jnp.maximum, FLOOR))
    tops = jnp.transpose(jnp.concatenate([top, jnp.zeros((120, 128), F32)], axis=0))
    top_out[...] = tops
    row = lax.broadcasted_iota(jnp.int32, (128, 128), 0)
    column = lax.broadcasted_iota(jnp.int32, (128, 128), 1)
    causal = row >= column
    for b in range(6):
        high = 128 * (b + 1)
        query = (kqv[128 * b : high, DQK : 2 * DQK].astype(F32) * DQK**-0.5).astype(BF16)
        scores = dot(query, kqv[0:high, 0:DQK], ((1,), (1,)))
        parts = []
        for u in range(b + 1):
            power = level[u : u + 1, :] - tops[:, b : b + 1]
            if u == b:
                power = jnp.where(causal, power, FLOOR)
            parts.append((scores[:, 128 * u : 128 * (u + 1)] * jnp.exp(power)).astype(BF16))
        weights = parts[0] if b == 0 else jnp.concatenate(parts, axis=1)
        local_out[128 * b : high, :] = dot(weights, kqv[0:high, 128:256])


def mixer_body(
    rows_in, w_outer, w_inner, w_signal, w_gate, aside, before,
    gate_out, conv_out, edge_out, rows, w_one, w_two, sems,
):
    loads = [
        pltpu.make_async_copy(w_outer, w_one.at[:, 0:128], sems.at[0]),
        pltpu.make_async_copy(w_inner, w_one.at[:, 128:256], sems.at[1]),
        pltpu.make_async_copy(rows_in, rows, sems.at[2]),
        pltpu.make_async_copy(w_signal, w_two.at[:, 0:128], sems.at[3]),
        pltpu.make_async_copy(w_gate, w_two.at[:, 128:256], sems.at[4]),
    ]
    for load in loads:
        load.start()
    for load in loads[0:3]:
        load.wait()
    first = dot(rows[...], w_one[...])
    outer = first[:, 0:128].astype(BF16).astype(F32)
    inner = first[:, 128:256].astype(BF16).astype(F32)
    for load in loads[3:5]:
        load.wait()
    second = dot(rows[...], w_two[...])
    signal = second[:, 0:128].astype(BF16).astype(F32)
    gate_out[...] = jax.nn.sigmoid(second[:, 128:256].astype(BF16).astype(F32)).astype(BF16)
    tap = aside[40:43, :]
    mixed = inner * signal
    at = lax.broadcasted_iota(jnp.int32, mixed.shape, 0)
    one = jnp.where(at >= 1, pltpu.roll(mixed, 1, 0), 0.0)
    two = jnp.where(at >= 2, pltpu.roll(mixed, 2, 0), 0.0)
    summed = tap[0:1] * two + tap[1:2] * one + tap[2:3] * mixed
    conv_out[...] = (outer * summed).astype(BF16)
    edge_out[0:16, :] = summed[0:16]
    edge_out[16:32, :] = outer[0:16]


def merged(states, peaks, decays, allowed, upto):
    scales = []
    after = jnp.zeros((1, 128), F32)
    for i in reversed(range(8)):
        scales.append(jnp.where(allowed[i], peaks[i] + after, FLOOR))
        after = after + jnp.where(upto[i], decays[i], 0.0)
    scales = scales[::-1]
    ceiling = functools.reduce(jnp.maximum, scales)
    total = jnp.zeros((DQK, DV), F32)
    for i in range(8):
        factor = jnp.where(allowed[i], jnp.exp(scales[i] - ceiling), 0.0)
        total = total + factor * states[i]
    return total, ceiling, after


def unpack(received):
    wide = [received[i].astype(F32) for i in range(8)]
    return (
        [w[0:64] for w in wide],
        [w[64:65] + w[65:66] + w[66:67] for w in wide],
        [w[67:68] + w[68:69] + w[69:70] for w in wide],
        [w[70:74] for w in wide],
    )


def line_body(received, tops, payload, before):
    me = own_sp() % 8
    states, peaks, decays, rims = unpack(received)
    every = [True] * 8
    state, peak, decay = merged(states, peaks, decays, every, every)
    packed = jnp.concatenate(
        [state] + split3(peak) + split3(decay) + [rims[7], jnp.zeros((PAYLOAD - 74, 128), F32)],
        axis=0,
    ).astype(BF16)
    for i in range(8):
        payload[i] = packed
    earlier = [i < me for i in range(8)]
    state, peak, decay = merged(states, peaks, decays, earlier, earlier)
    rim = jnp.zeros((4, 128), F32)
    for i in range(7):
        rim = jnp.where(me == i + 1, rims[i], rim)
    before[0:64, :] = state
    before[64:72, :] = jnp.concatenate([peak, decay, rim, jnp.zeros((2, 128), F32)], axis=0)


def final_body(
    received, aside, before_in, start_state, local_in, tops_in, gate_in, kqv_in, conv_in, edge_in,
    out, before, first_state, tops, local, out_gate, kqv, conv, edge, sems,
):
    head, y, z = own_tp(), own_sp() % 8, own_sp() // 8
    loads = [
        (start_state.at[head], first_state),
        (before_in, before),
        (tops_in, tops),
        (kqv_in.at[:, 0:128], kqv),
        (local_in, local),
        (gate_in, out_gate),
        (conv_in, conv),
        (edge_in, edge),
    ]
    loads = [pltpu.make_async_copy(a, b, sems.at[i]) for i, (a, b) in enumerate(loads)]
    for load in loads:
        load.start()
    states, peaks, decays, rims = unpack(received)
    earlier = [i < z for i in range(8)]
    state, peak, decay = merged(states, peaks, decays, earlier, earlier)
    lifted = aside[32:33, :] + decay
    ceiling = jnp.maximum(lifted, peak)
    loads[0].wait()
    state = jnp.exp(lifted - ceiling) * first_state[...] + jnp.exp(peak - ceiling) * state
    loads[1].wait()
    lifted = ceiling + before[65:66, :]
    peak = before[64:65, :]
    ceiling = jnp.maximum(lifted, peak)
    state = jnp.exp(lifted - ceiling) * state + jnp.exp(peak - ceiling) * before[0:64, :]
    state = (state * DQK**-0.5).astype(BF16)
    loads[2].wait()
    top = tops[...]
    best = jnp.maximum(top, ceiling)
    keep = jnp.exp(top - best)
    bring = jnp.exp(ceiling - best)
    for load in loads[3:]:
        load.wait()
    scale = aside[43:44, :]
    for b in range(6):
        here = slice(128 * b, 128 * (b + 1))
        remote = dot(kqv[here, DQK : 2 * DQK], state)
        number = bring[:, b : b + 1] * remote + keep[:, b : b + 1] * local[here, :]
        spread = lax.rsqrt(jnp.mean(number * number, axis=1, keepdims=True) + EPS)
        out[here, 128:256] = (number * spread * scale * out_gate[here, :].astype(F32)).astype(BF16)
    out[:, 0:128] = conv[...]
    rim = before[66:70, :]
    for i in range(7):
        rim = jnp.where(jnp.logical_and(y == 0, z == i + 1), rims[i], rim)
    past = rim[0:2] * rim[2:4]
    tap = aside[40:43, :]
    extra = jnp.concatenate(
        [tap[0:1] * past[0:1] + tap[1:2] * past[1:2], tap[0:1] * past[1:2], jnp.zeros((14, 128), F32)],
        axis=0,
    )
    out[0:16, 0:128] = (edge[16:32, :] * (edge[0:16, :] + extra)).astype(BF16)


def project_body(received, w0, w1, w2, w3, sent, kept, weights, sems):
    tp = own_tp()
    x, core = tp // 2, tp % 2
    loads = []
    for n in range(4):
        for i, weight in enumerate((w0, w3)):
            cut = pl.ds(512 * n, 512)
            loads.append(
                pltpu.make_async_copy(
                    weight.at[:, cut], weights.at[pl.ds(256 * i, 256), cut], sems.at[n, i]
                )
            )
    for load in loads:
        load.start()
    there = pl.ds(pl.multiple_of((1 - core) * 96, 32), 96)
    here = pl.ds(pl.multiple_of(core * 96, 32), 96)
    parts = [
        jnp.concatenate([received[(x + shift) % 4, rows, :] for rows in (there, here)], axis=0)
        for shift in (0, 3, 1, 2)
    ]
    for n in range(4):
        cut = slice(512 * n, 512 * (n + 1))
        total = dot(parts[1], w1[:, cut]) + dot(parts[2], w2[:, cut])
        for load in loads[2 * n : 2 * n + 2]:
            load.wait()
        total = total + dot(parts[0], weights[0:256, cut]) + dot(parts[3], weights[256:512, cut])
        sent[:, cut] = total[0:96].astype(BF16)
        kept[:, cut] = total[96:192]


def add_body(one, other, out):
    out[...] = (one[...] + other[...].astype(F32)).astype(BF16)


def tp_moves(move):
    moves = []
    for i in range(8):
        x, core = move(i // 2, i % 2)
        moves.append((i, (x % 4) * 2 + core))
    return moves


UP = tp_moves(lambda x, c: (x + 1, c))
DOWN = tp_moves(lambda x, c: (x - 1, c))
ACROSS = tp_moves(lambda x, c: (x + 2, c))
SWAP = tp_moves(lambda x, c: (x, 1 - c))
X_GROUPS = [[0, 2, 4, 6], [1, 3, 5, 7]]
Y_GROUPS = [[z * 8 + y for y in range(8)] for z in range(8)]
Z_GROUPS = [[z * 8 + y for z in range(8)] for y in range(8)]


def move(value, pairs):
    return lax.ppermute(value, "tp", pairs)


def to_all(copies, groups):
    return lax.all_to_all(copies, "sp", 0, 0, axis_index_groups=groups)


def on_device(
    tokens, input_norm_gain, w_outer, w_inner, w_signal, taps, w_query, w_key, w_value, w_gate,
    w_input, w_forget, in_bias, forget_bias, factor, extra, start_state, start_scale, head_gain,
    w_conv_out, w_memory_out,
):
    normed = call(
        norm_body, [("vmem", (96, 2048), BF16)], tag("load", tokens, input_norm_gain)
    )
    *prepared, w_out, aside = call(
        prepare_body,
        [
            ("vmem", (256, 2048), BF16),
            ("vmem", (2048, 128), BF16),
            ("vmem", (2048, 256), BF16),
            ("vmem", (256, 2048), BF16),
            ("vmem", (48, 128), F32),
        ],
        tag("smem", in_bias, forget_bias, start_scale)
        + tag("vmem", normed)
        + tag("hbm", w_key.T, w_query.T, w_input.T, w_forget.T, w_value, w_inner, w_signal)
        + tag("hbm", w_conv_out, w_memory_out)
        + tag("load", factor, extra.T, taps, head_gain),
        [pltpu.SemaphoreType.DMA((9,))],
    )
    low = move(normed, UP)
    far = move(normed, ACROSS)
    high = move(normed, DOWN)
    low, _ = lax.optimization_barrier((low, aside))
    near = call(stack_body, [("vmem", (288, 2048), BF16)], tag("vmem", normed, low, high))
    blocks = [normed, low, high, far, move(near, SWAP), move(far, SWAP)]

    w_sent = w_out
    w_up = move(w_sent, UP)
    w_down = move(w_sent, DOWN)

    payload, kqv, level, rows = call(
        state_body,
        [
            ("vmem", (8, PAYLOAD, 128), BF16),
            ("hbm", (768, 256), BF16),
            ("hbm", (8, 128), F32),
            ("hbm", (768, 2048), BF16),
        ],
        tag("vmem", *blocks, *prepared, aside),
        [
            pltpu.VMEM((768, 2048), BF16),
            pltpu.VMEM((768, 256), BF16),
            pltpu.VMEM((8, 128), F32),
            pltpu.SemaphoreType.DMA((3,)),
        ],
    )
    received = to_all(payload, Y_GROUPS)
    local, tops = call(
        local_body,
        [("load", (768, 128), F32), ("load", (128, 128), F32)],
        tag("load", level, kqv),
        flops=10**9,
    )
    payload, before = call(
        line_body,
        [("vmem", (8, PAYLOAD, 128), BF16), ("load", (72, 128), F32)],
        tag("vmem", received) + tag("hbm", tops),
    )
    w_far = w_out
    w_far = move(w_far, ACROSS)
    received = to_all(payload, Z_GROUPS)
    out_gate, conv, edge = call(
        mixer_body,
        [("load", (768, 128), BF16), ("load", (768, 128), BF16), ("load", (32, 128), F32)],
        tag("hbm", rows, w_outer, w_inner, w_signal, w_gate)
        + tag("vmem", aside)
        + tag("hbm", before),
        [
            pltpu.VMEM((768, 2048), BF16),
            pltpu.VMEM((2048, 256), BF16),
            pltpu.VMEM((2048, 256), BF16),
            pltpu.SemaphoreType.DMA((5,)),
        ],
        flops=10**9,
    )
    both = call(
        final_body,
        [("vmem", (768, 256), BF16)],
        tag("vmem", received, aside)
        + tag("hbm", before, start_state, local, tops, out_gate, kqv, conv, edge),
        [
            pltpu.VMEM((72, 128), F32),
            pltpu.VMEM((64, 128), F32),
            pltpu.VMEM((128, 128), F32),
            pltpu.VMEM((768, 128), F32),
            pltpu.VMEM((768, 128), BF16),
            pltpu.VMEM((768, 128), BF16),
            pltpu.VMEM((768, 128), BF16),
            pltpu.VMEM((32, 128), F32),
            pltpu.SemaphoreType.DMA((8,)),
        ],
    )
    mixers = lax.all_to_all(both.reshape(4, 192, 256), "tp", 0, 0, axis_index_groups=X_GROUPS)
    sent, kept = call(
        project_body,
        [("vmem", (96, 2048), BF16), ("vmem", (96, 2048), F32)],
        tag("vmem", mixers) + tag("hbm", w_out) + tag("vmem", w_up, w_down) + tag("hbm", w_far),
        [pltpu.VMEM((512, 2048), BF16), pltpu.SemaphoreType.DMA((4, 2))],
    )
    other = move(sent, SWAP)
    return call(add_body, [("load", (96, 2048), BF16)], tag("vmem", kept, other))


def solution(mesh):
    in_specs = (
        P(("sp", "tp"), None),
        P(),
        P(None, "tp"),
        P(None, "tp"),
        P(None, "tp"),
        P(),
        P(None, "tp"),
        P(None, "tp"),
        P(None, "tp"),
        P(None, "tp"),
        P(),
        P(),
        P(),
        P(),
        P("sp"),
        P("sp", None),
        P(),
        P(),
        P(),
        P("tp", None),
        P("tp", None),
    )

    return jax.shard_map(
        on_device,
        mesh=mesh,
        in_specs=in_specs,
        out_specs=P(("sp", "tp"), None),
        check_vma=False,
    )
```

```python
import functools

import jax
import jax.numpy as jnp
from jax import lax
from jax.experimental import pallas as pl
from jax.experimental.pallas import tpu as pltpu
from jax.sharding import PartitionSpec as P


DQK = 64
DV = 128
EPS = 1e-06
FLOOR = -1e30
F32 = jnp.float32
BF16 = jnp.bfloat16
PAYLOAD = 72

SPACES = {
    "vmem": (pltpu.VMEM, pltpu.VMEM),
    "hbm": (pltpu.HBM, pltpu.HBM),
    "load": (pltpu.HBM, pltpu.VMEM),
    "smem": (pltpu.HBM, pltpu.SMEM),
}


def call(body, outs, ins, scratch=(), flops=10**8, limit=16 << 20):
    results = pl.pallas_call(
        body,
        out_shape=tuple(SPACES[how][0](shape, kind) for how, shape, kind in outs),
        in_specs=[pl.BlockSpec(memory_space=SPACES[how][1]) for how, _ in ins],
        out_specs=tuple(pl.BlockSpec(memory_space=SPACES[how][1]) for how, _, _ in outs),
        scratch_shapes=list(scratch),
        compiler_params=pltpu.CompilerParams(vmem_limit_bytes=limit),
        cost_estimate=pl.CostEstimate(flops=flops, bytes_accessed=1 << 20, transcendentals=0),
    )(*[pltpu.with_memory_space_constraint(array, SPACES[how][0]) for how, array in ins])
    return results[0] if len(outs) == 1 else results


def tag(how, *arrays):
    return [(how, array) for array in arrays]


def dot(a, b, dims=((1,), (0,))):
    return lax.dot_general(a, b, (dims, ((), ())), preferred_element_type=F32)


def norm_body(tokens, gain, out):
    wide = tokens[...].astype(F32)
    scale = lax.rsqrt(jnp.mean(wide * wide, axis=1, keepdims=True) + EPS)
    out[...] = (wide * scale * gain[...].astype(F32).reshape(1, 2048)).astype(BF16)


def own_tp():
    return lax.axis_index("tp").astype(jnp.int32)


def own_sp():
    return lax.axis_index("sp").astype(jnp.int32)


def places(tp):
    x, core = tp // 2, tp % 2
    return [
        ((x + shift) % 4) * 2 + (1 - core if swapped else core)
        for swapped in (0, 1)
        for shift in (0, 3, 1, 2)
    ]


def stack_body(b0, b1, b2, out):
    out[0:96, :] = b0[...]
    out[96:192, :] = b1[...]
    out[192:288, :] = b2[...]


def split3(value):
    high = value.astype(BF16).astype(F32)
    rest = value - high
    middle = rest.astype(BF16).astype(F32)
    return [high, middle, rest - middle]


def packed(state, peak, decay, rim):
    lane = lax.broadcasted_iota(jnp.int32, (1, 128), 1)
    scales = jnp.zeros((1, 128), F32)
    for i, term in enumerate(split3(peak) + split3(decay)):
        scales = jnp.where(lane == i, term, scales)
    rows = [state, scales, rim, jnp.zeros((PAYLOAD - 69, 128), F32)]
    return jnp.concatenate(rows, axis=0).astype(BF16)


def lane_scan(value, op, neutral):
    lane = lax.broadcasted_iota(jnp.int32, value.shape, 1)
    step = 1
    while step < 128:
        value = op(value, jnp.where(lane >= step, pltpu.roll(value, step, 1), neutral))
        step *= 2
    return value


def row_scan(value, op, neutral):
    last = jnp.broadcast_to(value[:, 127:128], value.shape)
    row = lax.broadcasted_iota(jnp.int32, value.shape, 0)
    before = jnp.where(row >= 1, pltpu.roll(last, 1, 0), neutral)
    for step in (1, 2, 4):
        before = op(before, jnp.where(row >= step, pltpu.roll(before, step, 0), neutral))
    return before


def rows_of(wide_row):
    pieces = [wide_row[:, 128 * b : 128 * (b + 1)] for b in range(6)]
    return jnp.concatenate(pieces + [jnp.zeros((2, 128), F32)], axis=0)


def prepare_body(
    in_bias, forget_bias, start_scale, normed, w_key, w_query, w_input, w_forget, w_value,
    w_inner, w_signal, w_conv, w_memory, factor, extra, taps, gain,
    w_turned, w_value_out, w_rim, w_out, aside, sems,
):
    loads = [
        (w_key, w_turned.at[0:64, :]),
        (w_query, w_turned.at[64:128, :]),
        (w_input, w_turned.at[128:136, :]),
        (w_forget, w_turned.at[136:144, :]),
        (w_value, w_value_out),
        (w_inner, w_rim.at[:, 0:128]),
        (w_signal, w_rim.at[:, 128:256]),
        (w_conv, w_out.at[0:128, :]),
        (w_memory, w_out.at[128:256, :]),
    ]
    loads = [pltpu.make_async_copy(a, b, sems.at[i]) for i, (a, b) in enumerate(loads)]
    for load in loads:
        load.start()
    head = own_tp()
    w_turned[144:256, :] = jnp.zeros((112, 2048), BF16)
    aside[0:8, :] = rows_of(factor[...].reshape(1, 768))
    aside[8:16, :] = rows_of(extra[pl.ds(head, 1), :])
    aside[16:24, :] = jnp.full((8, 128), in_bias[head], F32)
    aside[24:32, :] = jnp.full((8, 128), forget_bias[head], F32)
    aside[32:40, :] = jnp.full((8, 128), start_scale[head], F32)
    lanes = pl.ds(pl.multiple_of(head * 128, 128), 128)
    gains = gain[...].astype(F32).reshape(1, 1024)
    own_gain = jnp.zeros((1, 128), F32)
    for i in range(8):
        own_gain = jnp.where(head == i, gains[:, 128 * i : 128 * (i + 1)], own_gain)
    aside[40:48, :] = jnp.concatenate(
        [taps[:, lanes].astype(F32), own_gain, jnp.zeros((4, 128), F32)], axis=0
    )
    for load in loads:
        load.wait()


def state_body(
    b0, b1, b2, b3, twins, b7, w_turned, w_value, w_rim, aside,
    payload, kqv_out, level_out, rows_out, rows, kqv, level_keep, sems,
):
    head = own_tp()
    blocks = [b0, b1, b2, b3] + [twins.at[pl.ds(96 * i, 96), :] for i in range(3)] + [b7]
    for place, block in zip(places(head), blocks):
        rows[pl.ds(pl.multiple_of(place * 96, 32), 96), :] = block[...]
    savings = [
        pltpu.make_async_copy(rows, rows_out, sems.at[0]),
        pltpu.make_async_copy(kqv, kqv_out, sems.at[1]),
        pltpu.make_async_copy(level_keep, level_out, sems.at[2]),
    ]
    savings[0].start()
    first = dot(rows[...], w_turned[...], ((1,), (1,)))
    values = dot(rows[...], w_value[...]).astype(BF16)
    rim = dot(rows[752:768, :], w_rim[...])
    turned = [jnp.transpose(first[128 * b : 128 * (b + 1), 128:256]) for b in range(6)]
    mine = lax.broadcasted_iota(jnp.int32, (8, 128), 0) == head
    pick = lambda part: jnp.sum(jnp.where(mine, part, 0.0), axis=0, keepdims=True)
    blank = jnp.zeros((2, 128), F32)
    log_input = jnp.concatenate([pick(t[0:8]) for t in turned] + [blank], axis=0) + aside[16:24, :]
    forget = jnp.concatenate([pick(t[8:16]) for t in turned] + [blank], axis=0) + aside[24:32, :]
    log_sig = jnp.minimum(forget, 0.0) - jnp.log1p(jnp.exp(-jnp.abs(forget)))
    log_forget = aside[0:8, :] * log_sig + aside[8:16, :]
    real = lax.broadcasted_iota(jnp.int32, (8, 128), 0) < 6
    until = lax.broadcasted_iota(jnp.int32, (128, 128), 0)
    until = (until <= lax.broadcasted_iota(jnp.int32, (128, 128), 1)).astype(F32)
    cumul = lax.dot_general(
        jnp.where(real, log_forget, 0.0),
        until,
        (((1,), (0,)), ((), ())),
        precision=lax.Precision.HIGHEST,
        preferred_element_type=F32,
    )
    cumul = cumul + row_scan(cumul, jnp.add, 0.0)
    level = jnp.where(real, log_input - cumul, FLOOR)
    total = cumul[5:6, 127:128]
    highest = jnp.max(level, keepdims=True)
    peak = jnp.broadcast_to(total + highest, (1, 128))
    weight = jnp.exp(level - highest)
    columns = jnp.transpose(jnp.concatenate([weight, jnp.zeros((120, 128), F32)], axis=0))
    kqv[:, 0:128] = first[:, 0:128].astype(BF16)
    kqv[:, 128:256] = values
    savings[1].start()
    level_keep[...] = level
    savings[2].start()
    pieces = []
    for b in range(6):
        keys = first[128 * b : 128 * (b + 1), 0:DQK].astype(BF16).astype(F32)
        pieces.append((keys * columns[:, b : b + 1]).astype(BF16))
    state = dot(jnp.concatenate(pieces, axis=0), values, ((0,), (0,)))
    rims = jnp.concatenate([rim[14:16, 0:128], rim[14:16, 128:256]], axis=0)
    sent = packed(state, peak, jnp.broadcast_to(total, (1, 128)), rims)
    for i in range(8):
        payload[i] = sent
    for saving in savings:
        saving.wait()


def local_body(level_in, kqv, local_out, top_out):
    level = level_in[...]
    top = lane_scan(level, jnp.maximum, FLOOR)
    top = jnp.maximum(top, row_scan(top, jnp.maximum, FLOOR))
    tops = jnp.transpose(jnp.concatenate([top, jnp.zeros((120, 128), F32)], axis=0))
    top_out[...] = tops
    row = lax.broadcasted_iota(jnp.int32, (128, 128), 0)
    column = lax.broadcasted_iota(jnp.int32, (128, 128), 1)
    causal = row >= column
    for b in range(6):
        high = 128 * (b + 1)
        query = (kqv[128 * b : high, DQK : 2 * DQK].astype(F32) * DQK**-0.5).astype(BF16)
        scores = dot(query, kqv[0:high, 0:DQK], ((1,), (1,)))
        parts = []
        for u in range(b + 1):
            power = level[u : u + 1, :] - tops[:, b : b + 1]
            if u == b:
                power = jnp.where(causal, power, FLOOR)
            parts.append((scores[:, 128 * u : 128 * (u + 1)] * jnp.exp(power)).astype(BF16))
        weights = parts[0] if b == 0 else jnp.concatenate(parts, axis=1)
        local_out[128 * b : high, :] = dot(weights, kqv[0:high, 128:256]).astype(BF16)


def mixer_body(
    rows_in, w_outer, w_inner, w_signal, w_gate, aside, before_in, start_state, local_in, tops_in,
    kqv_in, gate_out, conv_out, edge_out, before, first_state, tops, local, query,
    rows, w_all, sems,
):
    loads = [
        pltpu.make_async_copy(w_outer, w_all.at[:, 0:128], sems.at[0]),
        pltpu.make_async_copy(w_inner, w_all.at[:, 128:256], sems.at[1]),
        pltpu.make_async_copy(rows_in, rows, sems.at[2]),
        pltpu.make_async_copy(w_signal, w_all.at[:, 256:384], sems.at[3]),
        pltpu.make_async_copy(w_gate, w_all.at[:, 384:512], sems.at[4]),
        pltpu.make_async_copy(before_in, before, sems.at[5]),
        pltpu.make_async_copy(start_state.at[own_tp()], first_state, sems.at[6]),
        pltpu.make_async_copy(tops_in, tops, sems.at[7]),
        pltpu.make_async_copy(local_in, local, sems.at[8]),
        pltpu.make_async_copy(kqv_in.at[:, 0:128], query, sems.at[9]),
    ]
    for load in loads:
        load.start()
    for load in loads[0:5]:
        load.wait()
    first = dot(rows[...], w_all[:, 0:256])
    second = dot(rows[...], w_all[:, 256:512])
    outer = first[:, 0:128].astype(BF16).astype(F32)
    inner = first[:, 128:256].astype(BF16).astype(F32)
    signal = second[:, 0:128].astype(BF16).astype(F32)
    gate_out[...] = jax.nn.sigmoid(second[:, 128:256].astype(BF16).astype(F32)).astype(BF16)
    tap = aside[40:43, :]
    mixed = inner * signal
    at = lax.broadcasted_iota(jnp.int32, mixed.shape, 0)
    one = jnp.where(at >= 1, pltpu.roll(mixed, 1, 0), 0.0)
    two = jnp.where(at >= 2, pltpu.roll(mixed, 2, 0), 0.0)
    summed = tap[0:1] * two + tap[1:2] * one + tap[2:3] * mixed
    conv_out[...] = (outer * summed).astype(BF16)
    edge_out[0:16, :] = summed[0:16]
    edge_out[16:32, :] = outer[0:16]
    for load in loads[5:]:
        load.wait()


def merged(states, peaks, decays, allowed, upto):
    scales = []
    after = jnp.zeros((1, 128), F32)
    for i in reversed(range(8)):
        scales.append(jnp.where(allowed[i], peaks[i] + after, FLOOR))
        after = after + jnp.where(upto[i], decays[i], 0.0)
    scales = scales[::-1]
    ceiling = functools.reduce(jnp.maximum, scales)
    total = jnp.zeros((DQK, DV), F32)
    for i in range(8):
        factor = jnp.where(allowed[i], jnp.exp(scales[i] - ceiling), 0.0)
        total = total + factor * states[i]
    return total, ceiling, after


def unpack(received):
    wide = [received[(i + 4) % 8].astype(F32) for i in range(8)]
    scales = jnp.concatenate([w[64:65] for w in wide], axis=0)
    scales = scales + pltpu.roll(scales, 127, 1) + pltpu.roll(scales, 126, 1)
    peaks = jnp.broadcast_to(scales[:, 0:1], (8, 128))
    decays = jnp.broadcast_to(scales[:, 3:4], (8, 128))
    return (
        [w[0:64] for w in wide],
        [peaks[i : i + 1] for i in range(8)],
        [decays[i : i + 1] for i in range(8)],
        [w[65:69] for w in wide],
    )


def line_body(received, tops, payload, before):
    me = own_sp() % 8
    states, peaks, decays, rims = unpack(received)
    every = [True] * 8
    state, peak, decay = merged(states, peaks, decays, every, every)
    sent = packed(state, peak, decay, rims[7])
    for i in range(8):
        payload[i] = sent
    earlier = [i < me for i in range(8)]
    state, peak, decay = merged(states, peaks, decays, earlier, earlier)
    rim = jnp.zeros((4, 128), F32)
    for i in range(7):
        rim = jnp.where(me == i + 1, rims[i], rim)
    before[0:64, :] = state
    before[64:72, :] = jnp.concatenate([peak, decay, rim, jnp.zeros((2, 128), F32)], axis=0)


def final_body(
    received, aside, out_gate, conv, edge, before, first_state, tops, local, kqv, out
):
    y, z = own_sp() % 8, own_sp() // 8
    states, peaks, decays, rims = unpack(received)
    earlier = [i < z for i in range(8)]
    state, peak, decay = merged(states, peaks, decays, earlier, earlier)
    lifted = aside[32:33, :] + decay
    ceiling = jnp.maximum(lifted, peak)
    state = jnp.exp(lifted - ceiling) * first_state[...] + jnp.exp(peak - ceiling) * state
    lifted = ceiling + before[65:66, :]
    peak = before[64:65, :]
    ceiling = jnp.maximum(lifted, peak)
    state = jnp.exp(lifted - ceiling) * state + jnp.exp(peak - ceiling) * before[0:64, :]
    state = (state * DQK**-0.5).astype(BF16)
    top = tops[...]
    best = jnp.maximum(top, ceiling)
    keep = jnp.exp(top - best)
    bring = jnp.exp(ceiling - best)
    scale = aside[43:44, :]
    for b in range(6):
        here = slice(128 * b, 128 * (b + 1))
        remote = dot(kqv[here, DQK : 2 * DQK], state)
        number = bring[:, b : b + 1] * remote + keep[:, b : b + 1] * local[here, :].astype(F32)
        spread = lax.rsqrt(jnp.mean(number * number, axis=1, keepdims=True) + EPS)
        out[here, 128:256] = (number * spread * scale * out_gate[here, :].astype(F32)).astype(BF16)
    out[:, 0:128] = conv[...]
    rim = before[66:70, :]
    for i in range(7):
        rim = jnp.where(jnp.logical_and(y == 0, z == i + 1), rims[i], rim)
    past = rim[0:2] * rim[2:4]
    tap = aside[40:43, :]
    extra = jnp.concatenate(
        [tap[0:1] * past[0:1] + tap[1:2] * past[1:2], tap[0:1] * past[1:2], jnp.zeros((14, 128), F32)],
        axis=0,
    )
    out[0:16, 0:128] = (edge[16:32, :] * (edge[0:16, :] + extra)).astype(BF16)


def project_body(received, w0, w1, w2, w3, sent, kept, weights, sems):
    tp = own_tp()
    x, core = tp // 2, tp % 2
    loads = []
    for n in range(4):
        for i, weight in enumerate((w0, w2, w3)):
            cut = pl.ds(512 * n, 512)
            loads.append(
                pltpu.make_async_copy(
                    weight.at[:, cut], weights.at[pl.ds(256 * i, 256), cut], sems.at[n, i]
                )
            )
    for load in loads:
        load.start()
    there = pl.ds(pl.multiple_of((1 - core) * 96, 32), 96)
    here = pl.ds(pl.multiple_of(core * 96, 32), 96)
    both = jnp.concatenate(
        [
            jnp.concatenate([received[(x + shift) % 4, rows, :] for shift in (0, 1, 2)], axis=1)
            for rows in (there, here)
        ],
        axis=0,
    )
    low = jnp.concatenate([received[(x + 3) % 4, rows, :] for rows in (there, here)], axis=0)
    for n in range(4):
        for load in loads[3 * n : 3 * n + 3]:
            load.wait()
        cut = slice(512 * n, 512 * (n + 1))
        total = dot(low, w1[:, cut]) + dot(both, weights[:, cut])
        sent[:, cut] = total[0:96].astype(BF16)
        kept[:, cut] = total[96:192]


def add_body(one, other, out):
    out[...] = (one[...] + other[...].astype(F32)).astype(BF16)


def tp_moves(move):
    moves = []
    for i in range(8):
        x, core = move(i // 2, i % 2)
        moves.append((i, (x % 4) * 2 + core))
    return moves


UP = tp_moves(lambda x, c: (x + 1, c))
DOWN = tp_moves(lambda x, c: (x - 1, c))
ACROSS = tp_moves(lambda x, c: (x + 2, c))
SWAP = tp_moves(lambda x, c: (x, 1 - c))
X_GROUPS = [[0, 2, 4, 6], [1, 3, 5, 7]]
TURN = (4, 5, 6, 7, 0, 1, 2, 3)
Y_GROUPS = [[z * 8 + y for y in TURN] for z in range(8)]
Z_GROUPS = [[z * 8 + y for z in TURN] for y in range(8)]


def move(value, pairs):
    return lax.ppermute(value, "tp", pairs)


def to_all(copies, groups):
    return lax.all_to_all(copies, "sp", 0, 0, axis_index_groups=groups)


def on_device(
    tokens, input_norm_gain, w_outer, w_inner, w_signal, taps, w_query, w_key, w_value, w_gate,
    w_input, w_forget, in_bias, forget_bias, factor, extra, start_state, start_scale, head_gain,
    w_conv_out, w_memory_out,
):
    normed = call(
        norm_body, [("vmem", (96, 2048), BF16)], tag("load", tokens, input_norm_gain)
    )
    *prepared, w_out, aside = call(
        prepare_body,
        [
            ("vmem", (256, 2048), BF16),
            ("vmem", (2048, 128), BF16),
            ("vmem", (2048, 256), BF16),
            ("vmem", (256, 2048), BF16),
            ("vmem", (48, 128), F32),
        ],
        tag("smem", in_bias, forget_bias, start_scale)
        + tag("vmem", normed)
        + tag("hbm", w_key.T, w_query.T, w_input.T, w_forget.T, w_value, w_inner, w_signal)
        + tag("hbm", w_conv_out, w_memory_out)
        + tag("load", factor, extra.T, taps, head_gain),
        [pltpu.SemaphoreType.DMA((9,))],
    )
    low = move(normed, UP)
    far = move(normed, ACROSS)
    high = move(normed, DOWN)
    low, _ = lax.optimization_barrier((low, aside))
    near = call(stack_body, [("vmem", (288, 2048), BF16)], tag("vmem", normed, low, high))
    blocks = [normed, low, high, far, move(near, SWAP), move(far, SWAP)]

    w_sent = w_out
    w_up = move(w_sent, UP)
    w_down = move(w_sent, DOWN)

    payload, kqv, level, rows = call(
        state_body,
        [
            ("vmem", (8, PAYLOAD, 128), BF16),
            ("hbm", (768, 256), BF16),
            ("hbm", (8, 128), F32),
            ("hbm", (768, 2048), BF16),
        ],
        tag("vmem", *blocks, *prepared, aside),
        [
            pltpu.VMEM((768, 2048), BF16),
            pltpu.VMEM((768, 256), BF16),
            pltpu.VMEM((8, 128), F32),
            pltpu.SemaphoreType.DMA((3,)),
        ],
    )
    received = to_all(payload, Y_GROUPS)
    local, tops = call(
        local_body,
        [("load", (768, 128), BF16), ("load", (128, 128), F32)],
        tag("load", level, kqv),
        flops=10**9,
    )
    payload, before = call(
        line_body,
        [("vmem", (8, PAYLOAD, 128), BF16), ("load", (72, 128), F32)],
        tag("vmem", received) + tag("hbm", tops),
    )
    w_far = w_out
    w_far = move(w_far, ACROSS)
    received = to_all(payload, Z_GROUPS)
    prefetched = call(
        mixer_body,
        [
            ("vmem", (768, 128), BF16),
            ("vmem", (768, 128), BF16),
            ("vmem", (32, 128), F32),
            ("vmem", (72, 128), F32),
            ("vmem", (64, 128), F32),
            ("vmem", (128, 128), F32),
            ("vmem", (768, 128), BF16),
            ("vmem", (768, 128), BF16),
        ],
        tag("hbm", rows, w_outer, w_inner, w_signal, w_gate)
        + tag("vmem", aside)
        + tag("hbm", before, start_state, local, tops, kqv),
        [
            pltpu.VMEM((768, 2048), BF16),
            pltpu.VMEM((2048, 512), BF16),
            pltpu.SemaphoreType.DMA((10,)),
        ],
        flops=10**9,
    )
    both = call(
        final_body, [("vmem", (768, 256), BF16)], tag("vmem", received, aside, *prefetched)
    )
    mixers = lax.all_to_all(both.reshape(4, 192, 256), "tp", 0, 0, axis_index_groups=X_GROUPS)
    sent, kept = call(
        project_body,
        [("vmem", (96, 2048), BF16), ("vmem", (96, 2048), F32)],
        tag("vmem", mixers) + tag("hbm", w_out) + tag("vmem", w_up) + tag("hbm", w_down, w_far),
        [pltpu.VMEM((768, 2048), BF16), pltpu.SemaphoreType.DMA((4, 3))],
    )
    other = move(sent, SWAP)
    return call(add_body, [("load", (96, 2048), BF16)], tag("vmem", kept, other))


def solution(mesh):
    in_specs = (
        P(("sp", "tp"), None),
        P(),
        P(None, "tp"),
        P(None, "tp"),
        P(None, "tp"),
        P(),
        P(None, "tp"),
        P(None, "tp"),
        P(None, "tp"),
        P(None, "tp"),
        P(),
        P(),
        P(),
        P(),
        P("sp"),
        P("sp", None),
        P(),
        P(),
        P(),
        P("tp", None),
        P("tp", None),
    )

    return jax.shard_map(
        on_device,
        mesh=mesh,
        in_specs=in_specs,
        out_specs=P(("sp", "tp"), None),
        check_vma=False,
    )
```

```python
import functools

import jax
import jax.numpy as jnp
from jax import lax
from jax.experimental import pallas as pl
from jax.experimental.pallas import tpu as pltpu
from jax.sharding import PartitionSpec as P


DQK = 64
DV = 128
EPS = 1e-06
FLOOR = -1e30
F32 = jnp.float32
BF16 = jnp.bfloat16
PAYLOAD = 72

SPACES = {
    "vmem": (pltpu.VMEM, pltpu.VMEM),
    "hbm": (pltpu.HBM, pltpu.HBM),
    "load": (pltpu.HBM, pltpu.VMEM),
    "smem": (pltpu.HBM, pltpu.SMEM),
}


def call(body, outs, ins, scratch=(), flops=10**8, limit=16 << 20):
    results = pl.pallas_call(
        body,
        out_shape=tuple(SPACES[how][0](shape, kind) for how, shape, kind in outs),
        in_specs=[pl.BlockSpec(memory_space=SPACES[how][1]) for how, _ in ins],
        out_specs=tuple(pl.BlockSpec(memory_space=SPACES[how][1]) for how, _, _ in outs),
        scratch_shapes=list(scratch),
        compiler_params=pltpu.CompilerParams(vmem_limit_bytes=limit),
        cost_estimate=pl.CostEstimate(flops=flops, bytes_accessed=1 << 20, transcendentals=0),
    )(*[pltpu.with_memory_space_constraint(array, SPACES[how][0]) for how, array in ins])
    return results[0] if len(outs) == 1 else results


def tag(how, *arrays):
    return [(how, array) for array in arrays]


def dot(a, b, dims=((1,), (0,))):
    return lax.dot_general(a, b, (dims, ((), ())), preferred_element_type=F32)


def norm_body(tokens, gain, out):
    wide = tokens[...].astype(F32)
    scale = lax.rsqrt(jnp.mean(wide * wide, axis=1, keepdims=True) + EPS)
    out[...] = (wide * scale * gain[...].astype(F32).reshape(1, 2048)).astype(BF16)


def own_tp():
    return lax.axis_index("tp").astype(jnp.int32)


def own_sp():
    return lax.axis_index("sp").astype(jnp.int32)


def places(tp):
    x, core = tp // 2, tp % 2
    return [
        ((x + shift) % 4) * 2 + (1 - core if swapped else core)
        for swapped in (0, 1)
        for shift in (0, 3, 1, 2)
    ]


def stack_body(b0, b1, b2, out):
    out[0:96, :] = b0[...]
    out[96:192, :] = b1[...]
    out[192:288, :] = b2[...]


def split3(value):
    high = value.astype(BF16).astype(F32)
    rest = value - high
    middle = rest.astype(BF16).astype(F32)
    return [high, middle, rest - middle]


def packed(state, peak, decay, rim):
    lane = lax.broadcasted_iota(jnp.int32, (1, 128), 1)
    scales = jnp.zeros((1, 128), F32)
    for i, term in enumerate(split3(peak) + split3(decay)):
        scales = jnp.where(lane == i, term, scales)
    rows = [state, scales, rim, jnp.zeros((PAYLOAD - 69, 128), F32)]
    return jnp.concatenate(rows, axis=0).astype(BF16)


def lane_scan(value, op, neutral):
    lane = lax.broadcasted_iota(jnp.int32, value.shape, 1)
    step = 1
    while step < 128:
        value = op(value, jnp.where(lane >= step, pltpu.roll(value, step, 1), neutral))
        step *= 2
    return value


def row_scan(value, op, neutral):
    last = jnp.broadcast_to(value[:, 127:128], value.shape)
    row = lax.broadcasted_iota(jnp.int32, value.shape, 0)
    before = jnp.where(row >= 1, pltpu.roll(last, 1, 0), neutral)
    for step in (1, 2, 4):
        before = op(before, jnp.where(row >= step, pltpu.roll(before, step, 0), neutral))
    return before


def rows_of(wide_row):
    pieces = [wide_row[:, 128 * b : 128 * (b + 1)] for b in range(6)]
    return jnp.concatenate(pieces + [jnp.zeros((2, 128), F32)], axis=0)


def prepare_body(
    normed, in_bias_in, forget_bias_in, start_scale_in, w_key, w_query, w_input, w_forget, w_value,
    w_inner, w_signal, w_conv, w_memory, factor_in, extra_in, taps_in, gain_in,
    w_turned, w_value_out, w_rim, w_out, aside,
    in_bias, forget_bias, start_scale, factor, extra, taps, gain, sems,
):
    loads = [
        (w_key, w_turned.at[0:64, :]),
        (w_query, w_turned.at[64:128, :]),
        (w_input, w_turned.at[128:136, :]),
        (w_forget, w_turned.at[136:144, :]),
        (w_value, w_value_out),
        (w_inner, w_rim.at[:, 0:128]),
        (w_signal, w_rim.at[:, 128:256]),
        (w_conv, w_out.at[0:128, :]),
        (w_memory, w_out.at[128:256, :]),
        (in_bias_in, in_bias),
        (forget_bias_in, forget_bias),
        (start_scale_in, start_scale),
        (factor_in, factor),
        (extra_in, extra),
        (taps_in, taps),
        (gain_in, gain),
    ]
    loads = [pltpu.make_async_copy(a, b, sems.at[i]) for i, (a, b) in enumerate(loads)]
    for load in loads:
        load.start()
    head = own_tp()
    for load in loads[9:]:
        load.wait()
    w_turned[144:256, :] = jnp.zeros((112, 2048), BF16)
    aside[0:8, :] = rows_of(factor[...].reshape(1, 768))
    aside[8:16, :] = rows_of(extra[pl.ds(head, 1), :])
    aside[16:24, :] = jnp.full((8, 128), in_bias[head], F32)
    aside[24:32, :] = jnp.full((8, 128), forget_bias[head], F32)
    aside[32:40, :] = jnp.full((8, 128), start_scale[head], F32)
    lanes = pl.ds(pl.multiple_of(head * 128, 128), 128)
    gains = gain[...].astype(F32).reshape(1, 1024)
    own_gain = jnp.zeros((1, 128), F32)
    for i in range(8):
        own_gain = jnp.where(head == i, gains[:, 128 * i : 128 * (i + 1)], own_gain)
    aside[40:48, :] = jnp.concatenate(
        [taps[:, lanes].astype(F32), own_gain, jnp.zeros((4, 128), F32)], axis=0
    )
    for load in loads[0:9]:
        load.wait()


def state_body(
    b0, b1, b2, b3, twins, b7, w_turned, w_value, w_rim, aside,
    payload, kqv_out, level_out, rows_out, rows, kqv, level_keep, sems,
):
    head = own_tp()
    blocks = [b0, b1, b2, b3] + [twins.at[pl.ds(96 * i, 96), :] for i in range(3)] + [b7]
    for place, block in zip(places(head), blocks):
        rows[pl.ds(pl.multiple_of(place * 96, 32), 96), :] = block[...]
    savings = [
        pltpu.make_async_copy(rows, rows_out, sems.at[0]),
        pltpu.make_async_copy(kqv, kqv_out, sems.at[1]),
        pltpu.make_async_copy(level_keep, level_out, sems.at[2]),
    ]
    savings[0].start()
    first = dot(rows[...], w_turned[...], ((1,), (1,)))
    values = dot(rows[...], w_value[...]).astype(BF16)
    rim = dot(rows[752:768, :], w_rim[...])
    turned = [jnp.transpose(first[128 * b : 128 * (b + 1), 128:256]) for b in range(6)]
    mine = lax.broadcasted_iota(jnp.int32, (8, 128), 0) == head
    pick = lambda part: jnp.sum(jnp.where(mine, part, 0.0), axis=0, keepdims=True)
    blank = jnp.zeros((2, 128), F32)
    log_input = jnp.concatenate([pick(t[0:8]) for t in turned] + [blank], axis=0) + aside[16:24, :]
    forget = jnp.concatenate([pick(t[8:16]) for t in turned] + [blank], axis=0) + aside[24:32, :]
    log_sig = jnp.minimum(forget, 0.0) - jnp.log1p(jnp.exp(-jnp.abs(forget)))
    log_forget = aside[0:8, :] * log_sig + aside[8:16, :]
    real = lax.broadcasted_iota(jnp.int32, (8, 128), 0) < 6
    until = lax.broadcasted_iota(jnp.int32, (128, 128), 0)
    until = (until <= lax.broadcasted_iota(jnp.int32, (128, 128), 1)).astype(F32)
    cumul = lax.dot_general(
        jnp.where(real, log_forget, 0.0),
        until,
        (((1,), (0,)), ((), ())),
        precision=lax.Precision.HIGHEST,
        preferred_element_type=F32,
    )
    cumul = cumul + row_scan(cumul, jnp.add, 0.0)
    level = jnp.where(real, log_input - cumul, FLOOR)
    total = cumul[5:6, 127:128]
    highest = jnp.max(level, keepdims=True)
    peak = jnp.broadcast_to(total + highest, (1, 128))
    weight = jnp.exp(level - highest)
    columns = jnp.transpose(jnp.concatenate([weight, jnp.zeros((120, 128), F32)], axis=0))
    kqv[:, 0:128] = first[:, 0:128].astype(BF16)
    kqv[:, 128:256] = values
    savings[1].start()
    level_keep[...] = level
    savings[2].start()
    pieces = []
    for b in range(6):
        keys = first[128 * b : 128 * (b + 1), 0:DQK].astype(BF16).astype(F32)
        pieces.append((keys * columns[:, b : b + 1]).astype(BF16))
    state = dot(jnp.concatenate(pieces, axis=0), values, ((0,), (0,)))
    rims = jnp.concatenate([rim[14:16, 0:128], rim[14:16, 128:256]], axis=0)
    sent = packed(state, peak, jnp.broadcast_to(total, (1, 128)), rims)
    for i in range(8):
        payload[i] = sent
    for saving in savings:
        saving.wait()


def local_body(level_in, kqv, local_out, top_out):
    level = level_in[...]
    top = lane_scan(level, jnp.maximum, FLOOR)
    top = jnp.maximum(top, row_scan(top, jnp.maximum, FLOOR))
    tops = jnp.transpose(jnp.concatenate([top, jnp.zeros((120, 128), F32)], axis=0))
    top_out[...] = tops
    row = lax.broadcasted_iota(jnp.int32, (128, 128), 0)
    column = lax.broadcasted_iota(jnp.int32, (128, 128), 1)
    causal = row >= column
    for b in range(6):
        high = 128 * (b + 1)
        query = (kqv[128 * b : high, DQK : 2 * DQK].astype(F32) * DQK**-0.5).astype(BF16)
        scores = dot(query, kqv[0:high, 0:DQK], ((1,), (1,)))
        parts = []
        for u in range(b + 1):
            power = level[u : u + 1, :] - tops[:, b : b + 1]
            if u == b:
                power = jnp.where(causal, power, FLOOR)
            parts.append((scores[:, 128 * u : 128 * (u + 1)] * jnp.exp(power)).astype(BF16))
        weights = parts[0] if b == 0 else jnp.concatenate(parts, axis=1)
        local_out[128 * b : high, :] = dot(weights, kqv[0:high, 128:256]).astype(BF16)


def mixer_body(
    rows_in, w_outer, w_inner, w_signal, w_gate, aside, before_in, start_state, local_in, tops_in,
    kqv_in, gate_out, conv_out, edge_out, before, first_state, tops, local, query,
    rows, w_all, sems,
):
    loads = [
        pltpu.make_async_copy(w_outer, w_all.at[:, 0:128], sems.at[0]),
        pltpu.make_async_copy(w_inner, w_all.at[:, 128:256], sems.at[1]),
        pltpu.make_async_copy(rows_in, rows, sems.at[2]),
        pltpu.make_async_copy(w_signal, w_all.at[:, 256:384], sems.at[3]),
        pltpu.make_async_copy(w_gate, w_all.at[:, 384:512], sems.at[4]),
        pltpu.make_async_copy(before_in, before, sems.at[5]),
        pltpu.make_async_copy(start_state.at[own_tp()], first_state, sems.at[6]),
        pltpu.make_async_copy(tops_in, tops, sems.at[7]),
        pltpu.make_async_copy(local_in, local, sems.at[8]),
        pltpu.make_async_copy(kqv_in.at[:, 0:128], query, sems.at[9]),
    ]
    for load in loads:
        load.start()
    for load in loads[0:5]:
        load.wait()
    first = dot(rows[...], w_all[:, 0:256])
    second = dot(rows[...], w_all[:, 256:512])
    outer = first[:, 0:128].astype(BF16).astype(F32)
    inner = first[:, 128:256].astype(BF16).astype(F32)
    signal = second[:, 0:128].astype(BF16).astype(F32)
    gate_out[...] = jax.nn.sigmoid(second[:, 128:256].astype(BF16).astype(F32)).astype(BF16)
    tap = aside[40:43, :]
    mixed = inner * signal
    at = lax.broadcasted_iota(jnp.int32, mixed.shape, 0)
    one = jnp.where(at >= 1, pltpu.roll(mixed, 1, 0), 0.0)
    two = jnp.where(at >= 2, pltpu.roll(mixed, 2, 0), 0.0)
    summed = tap[0:1] * two + tap[1:2] * one + tap[2:3] * mixed
    conv_out[...] = (outer * summed).astype(BF16)
    edge_out[0:16, :] = summed[0:16]
    edge_out[16:32, :] = outer[0:16]
    for load in loads[5:]:
        load.wait()


def merged(states, peaks, decays, allowed, upto):
    scales = []
    after = jnp.zeros((1, 128), F32)
    for i in reversed(range(8)):
        scales.append(jnp.where(allowed[i], peaks[i] + after, FLOOR))
        after = after + jnp.where(upto[i], decays[i], 0.0)
    scales = scales[::-1]
    ceiling = functools.reduce(jnp.maximum, scales)
    total = jnp.zeros((DQK, DV), F32)
    for i in range(8):
        factor = jnp.where(allowed[i], jnp.exp(scales[i] - ceiling), 0.0)
        total = total + factor * states[i]
    return total, ceiling, after


def unpack(received):
    wide = [received[(i + 4) % 8].astype(F32) for i in range(8)]
    scales = jnp.concatenate([w[64:65] for w in wide], axis=0)
    scales = scales + pltpu.roll(scales, 127, 1) + pltpu.roll(scales, 126, 1)
    peaks = jnp.broadcast_to(scales[:, 0:1], (8, 128))
    decays = jnp.broadcast_to(scales[:, 3:4], (8, 128))
    return (
        [w[0:64] for w in wide],
        [peaks[i : i + 1] for i in range(8)],
        [decays[i : i + 1] for i in range(8)],
        [w[65:69] for w in wide],
    )


def line_body(received, tops, payload, before):
    me = own_sp() % 8
    states, peaks, decays, rims = unpack(received)
    every = [True] * 8
    state, peak, decay = merged(states, peaks, decays, every, every)
    sent = packed(state, peak, decay, rims[7])
    for i in range(8):
        payload[i] = sent
    earlier = [i < me for i in range(8)]
    state, peak, decay = merged(states, peaks, decays, earlier, earlier)
    rim = jnp.zeros((4, 128), F32)
    for i in range(7):
        rim = jnp.where(me == i + 1, rims[i], rim)
    before[0:64, :] = state
    before[64:72, :] = jnp.concatenate([peak, decay, rim, jnp.zeros((2, 128), F32)], axis=0)


def final_body(
    received, aside, out_gate, conv, edge, before, first_state, tops, local, kqv, out
):
    y, z = own_sp() % 8, own_sp() // 8
    states, peaks, decays, rims = unpack(received)
    earlier = [i < z for i in range(8)]
    state, peak, decay = merged(states, peaks, decays, earlier, earlier)
    lifted = aside[32:33, :] + decay
    ceiling = jnp.maximum(lifted, peak)
    state = jnp.exp(lifted - ceiling) * first_state[...] + jnp.exp(peak - ceiling) * state
    lifted = ceiling + before[65:66, :]
    peak = before[64:65, :]
    ceiling = jnp.maximum(lifted, peak)
    state = jnp.exp(lifted - ceiling) * state + jnp.exp(peak - ceiling) * before[0:64, :]
    state = (state * DQK**-0.5).astype(BF16)
    top = tops[...]
    best = jnp.maximum(top, ceiling)
    keep = jnp.exp(top - best)
    bring = jnp.exp(ceiling - best)
    scale = aside[43:44, :]
    for b in range(6):
        here = slice(128 * b, 128 * (b + 1))
        remote = dot(kqv[here, DQK : 2 * DQK], state)
        number = bring[:, b : b + 1] * remote + keep[:, b : b + 1] * local[here, :].astype(F32)
        spread = lax.rsqrt(jnp.mean(number * number, axis=1, keepdims=True) + EPS)
        there = slice(128 * ((b + 3) % 6), 128 * ((b + 3) % 6) + 128)
        out[there, 128:256] = (number * spread * scale * out_gate[here, :].astype(F32)).astype(BF16)
    out[384:768, 0:128] = conv[0:384, :]
    out[0:384, 0:128] = conv[384:768, :]
    rim = before[66:70, :]
    for i in range(7):
        rim = jnp.where(jnp.logical_and(y == 0, z == i + 1), rims[i], rim)
    past = rim[0:2] * rim[2:4]
    tap = aside[40:43, :]
    extra = jnp.concatenate(
        [tap[0:1] * past[0:1] + tap[1:2] * past[1:2], tap[0:1] * past[1:2], jnp.zeros((14, 128), F32)],
        axis=0,
    )
    out[384:400, 0:128] = (edge[16:32, :] * (edge[0:16, :] + extra)).astype(BF16)


def project_body(received, w0, w1, w2, w3, sent, kept, weights, sems):
    tp = own_tp()
    x, core = tp // 2, tp % 2
    loads = []
    for n in range(4):
        for i, weight in enumerate((w0, w2, w3)):
            cut = pl.ds(512 * n, 512)
            loads.append(
                pltpu.make_async_copy(
                    weight.at[:, cut], weights.at[pl.ds(256 * i, 256), cut], sems.at[n, i]
                )
            )
    for load in loads:
        load.start()
    there = pl.ds(pl.multiple_of((1 - core) * 96, 32), 96)
    here = pl.ds(pl.multiple_of(core * 96, 32), 96)
    both = jnp.concatenate(
        [
            jnp.concatenate([received[(x + shift + 2) % 4, rows, :] for shift in (0, 1, 2)], axis=1)
            for rows in (there, here)
        ],
        axis=0,
    )
    low = jnp.concatenate([received[(x + 1) % 4, rows, :] for rows in (there, here)], axis=0)
    for n in range(4):
        for load in loads[3 * n : 3 * n + 3]:
            load.wait()
        cut = slice(512 * n, 512 * (n + 1))
        total = dot(low, w1[:, cut]) + dot(both, weights[:, cut])
        sent[:, cut] = total[0:96].astype(BF16)
        kept[:, cut] = total[96:192]


def add_body(one, other, out):
    out[...] = (one[...] + other[...].astype(F32)).astype(BF16)


def tp_moves(move):
    moves = []
    for i in range(8):
        x, core = move(i // 2, i % 2)
        moves.append((i, (x % 4) * 2 + core))
    return moves


UP = tp_moves(lambda x, c: (x + 1, c))
DOWN = tp_moves(lambda x, c: (x - 1, c))
ACROSS = tp_moves(lambda x, c: (x + 2, c))
SWAP = tp_moves(lambda x, c: (x, 1 - c))
X_GROUPS = [[4, 6, 0, 2], [5, 7, 1, 3]]
TURN = (4, 5, 6, 7, 0, 1, 2, 3)
Y_GROUPS = [[z * 8 + y for y in TURN] for z in range(8)]
Z_GROUPS = [[z * 8 + y for z in TURN] for y in range(8)]


def move(value, pairs):
    return lax.ppermute(value, "tp", pairs)


def to_all(copies, groups):
    return lax.all_to_all(copies, "sp", 0, 0, axis_index_groups=groups)


def on_device(
    tokens, input_norm_gain, w_outer, w_inner, w_signal, taps, w_query, w_key, w_value, w_gate,
    w_input, w_forget, in_bias, forget_bias, factor, extra, start_state, start_scale, head_gain,
    w_conv_out, w_memory_out,
):
    normed = call(
        norm_body, [("vmem", (96, 2048), BF16)], tag("load", tokens, input_norm_gain)
    )
    *prepared, w_out, aside = call(
        prepare_body,
        [
            ("vmem", (256, 2048), BF16),
            ("vmem", (2048, 128), BF16),
            ("vmem", (2048, 256), BF16),
            ("vmem", (256, 2048), BF16),
            ("vmem", (48, 128), F32),
        ],
        tag("vmem", normed)
        + tag("hbm", in_bias, forget_bias, start_scale)
        + tag("hbm", w_key.T, w_query.T, w_input.T, w_forget.T, w_value, w_inner, w_signal)
        + tag("hbm", w_conv_out, w_memory_out, factor, extra.T, taps, head_gain),
        [
            pltpu.SMEM((8,), F32),
            pltpu.SMEM((8,), F32),
            pltpu.SMEM((8,), F32),
            pltpu.VMEM((768,), F32),
            pltpu.VMEM((8, 768), F32),
            pltpu.VMEM((3, 1024), BF16),
            pltpu.VMEM((1024,), BF16),
            pltpu.SemaphoreType.DMA((16,)),
        ],
    )
    low = move(normed, UP)
    far = move(normed, ACROSS)
    high = move(normed, DOWN)
    low, _ = lax.optimization_barrier((low, aside))
    near = call(stack_body, [("vmem", (288, 2048), BF16)], tag("vmem", normed, low, high))
    blocks = [normed, low, high, far, move(near, SWAP), move(far, SWAP)]

    w_sent = w_out
    w_up = move(w_sent, UP)
    w_down = move(w_sent, DOWN)

    payload, kqv, level, rows = call(
        state_body,
        [
            ("vmem", (8, PAYLOAD, 128), BF16),
            ("hbm", (768, 256), BF16),
            ("hbm", (8, 128), F32),
            ("hbm", (768, 2048), BF16),
        ],
        tag("vmem", *blocks, *prepared, aside),
        [
            pltpu.VMEM((768, 2048), BF16),
            pltpu.VMEM((768, 256), BF16),
            pltpu.VMEM((8, 128), F32),
            pltpu.SemaphoreType.DMA((3,)),
        ],
    )
    received = to_all(payload, Y_GROUPS)
    local, tops = call(
        local_body,
        [("load", (768, 128), BF16), ("load", (128, 128), F32)],
        tag("load", level, kqv),
        flops=10**9,
    )
    payload, before = call(
        line_body,
        [("vmem", (8, PAYLOAD, 128), BF16), ("load", (72, 128), F32)],
        tag("vmem", received) + tag("hbm", tops),
    )
    w_far = w_out
    w_far = move(w_far, ACROSS)
    received = to_all(payload, Z_GROUPS)
    prefetched = call(
        mixer_body,
        [
            ("vmem", (768, 128), BF16),
            ("vmem", (768, 128), BF16),
            ("vmem", (32, 128), F32),
            ("vmem", (72, 128), F32),
            ("vmem", (64, 128), F32),
            ("vmem", (128, 128), F32),
            ("vmem", (768, 128), BF16),
            ("vmem", (768, 128), BF16),
        ],
        tag("hbm", rows, w_outer, w_inner, w_signal, w_gate)
        + tag("vmem", aside)
        + tag("hbm", before, start_state, local, tops, kqv),
        [
            pltpu.VMEM((768, 2048), BF16),
            pltpu.VMEM((2048, 512), BF16),
            pltpu.SemaphoreType.DMA((10,)),
        ],
        flops=10**9,
    )
    both = call(
        final_body, [("vmem", (768, 256), BF16)], tag("vmem", received, aside, *prefetched)
    )
    mixers = lax.all_to_all(both.reshape(4, 192, 256), "tp", 0, 0, axis_index_groups=X_GROUPS)
    sent, kept = call(
        project_body,
        [("vmem", (96, 2048), BF16), ("vmem", (96, 2048), F32)],
        tag("vmem", mixers) + tag("hbm", w_out) + tag("vmem", w_up) + tag("hbm", w_down, w_far),
        [pltpu.VMEM((768, 2048), BF16), pltpu.SemaphoreType.DMA((4, 3))],
    )
    other = move(sent, SWAP)
    return call(add_body, [("load", (96, 2048), BF16)], tag("vmem", kept, other))


def solution(mesh):
    in_specs = (
        P(("sp", "tp"), None),
        P(),
        P(None, "tp"),
        P(None, "tp"),
        P(None, "tp"),
        P(),
        P(None, "tp"),
        P(None, "tp"),
        P(None, "tp"),
        P(None, "tp"),
        P(),
        P(),
        P(),
        P(),
        P("sp"),
        P("sp", None),
        P(),
        P(),
        P(),
        P("tp", None),
        P("tp", None),
    )

    return jax.shard_map(
        on_device,
        mesh=mesh,
        in_specs=in_specs,
        out_specs=P(("sp", "tp"), None),
        check_vma=False,
    )
```

```python
import functools

import jax
import jax.numpy as jnp
from jax import lax
from jax.experimental import pallas as pl
from jax.experimental.pallas import tpu as pltpu
from jax.sharding import PartitionSpec as P


DQK = 64
DV = 128
EPS = 1e-06
FLOOR = -1e30
F32 = jnp.float32
BF16 = jnp.bfloat16
PAYLOAD = 72

SPACES = {
    "vmem": (pltpu.VMEM, pltpu.VMEM),
    "hbm": (pltpu.HBM, pltpu.HBM),
    "load": (pltpu.HBM, pltpu.VMEM),
    "smem": (pltpu.HBM, pltpu.SMEM),
}


def call(body, outs, ins, scratch=(), flops=10**8, limit=16 << 20):
    results = pl.pallas_call(
        body,
        out_shape=tuple(SPACES[how][0](shape, kind) for how, shape, kind in outs),
        in_specs=[pl.BlockSpec(memory_space=SPACES[how][1]) for how, _ in ins],
        out_specs=tuple(pl.BlockSpec(memory_space=SPACES[how][1]) for how, _, _ in outs),
        scratch_shapes=list(scratch),
        compiler_params=pltpu.CompilerParams(vmem_limit_bytes=limit),
        cost_estimate=pl.CostEstimate(flops=flops, bytes_accessed=1 << 20, transcendentals=0),
    )(*[pltpu.with_memory_space_constraint(array, SPACES[how][0]) for how, array in ins])
    return results[0] if len(outs) == 1 else results


def tag(how, *arrays):
    return [(how, array) for array in arrays]


def dot(a, b, dims=((1,), (0,))):
    return lax.dot_general(a, b, (dims, ((), ())), preferred_element_type=F32)


def norm_body(tokens_in, gain_in, out, tokens, gain, sems):
    loads = [
        pltpu.make_async_copy(tokens_in, tokens, sems.at[0]),
        pltpu.make_async_copy(gain_in, gain, sems.at[1]),
    ]
    for load in loads:
        load.start()
    for load in loads:
        load.wait()
    wide = tokens[...].astype(F32)
    scale = lax.rsqrt(jnp.mean(wide * wide, axis=1, keepdims=True) + EPS)
    out[...] = (wide * scale * gain[...].astype(F32).reshape(1, 2048)).astype(BF16)


def own_tp():
    return lax.axis_index("tp").astype(jnp.int32)


def own_sp():
    return lax.axis_index("sp").astype(jnp.int32)


def places(tp):
    x, core = tp // 2, tp % 2
    return [
        ((x + shift) % 4) * 2 + (1 - core if swapped else core)
        for swapped in (0, 1)
        for shift in (0, 3, 1, 2)
    ]


def stack_body(b0, b1, b2, out):
    out[0:96, :] = b0[...]
    out[96:192, :] = b1[...]
    out[192:288, :] = b2[...]


def split3(value):
    high = value.astype(BF16).astype(F32)
    rest = value - high
    middle = rest.astype(BF16).astype(F32)
    return [high, middle, rest - middle]


def packed(state, peak, decay, rim):
    lane = lax.broadcasted_iota(jnp.int32, (1, 128), 1)
    scales = jnp.zeros((1, 128), F32)
    for i, term in enumerate(split3(peak) + split3(decay)):
        scales = jnp.where(lane == i, term, scales)
    rows = [state, scales, rim, jnp.zeros((PAYLOAD - 69, 128), F32)]
    return jnp.concatenate(rows, axis=0).astype(BF16)


def lane_scan(value, op, neutral):
    lane = lax.broadcasted_iota(jnp.int32, value.shape, 1)
    step = 1
    while step < 128:
        value = op(value, jnp.where(lane >= step, pltpu.roll(value, step, 1), neutral))
        step *= 2
    return value


def row_scan(value, op, neutral):
    last = jnp.broadcast_to(value[:, 127:128], value.shape)
    row = lax.broadcasted_iota(jnp.int32, value.shape, 0)
    before = jnp.where(row >= 1, pltpu.roll(last, 1, 0), neutral)
    for step in (1, 2, 4):
        before = op(before, jnp.where(row >= step, pltpu.roll(before, step, 0), neutral))
    return before


def rows_of(wide_row):
    pieces = [wide_row[:, 128 * b : 128 * (b + 1)] for b in range(6)]
    return jnp.concatenate(pieces + [jnp.zeros((2, 128), F32)], axis=0)


def prepare_body(
    normed, in_bias_in, forget_bias_in, start_scale_in, w_key, w_query, w_input, w_forget, w_value,
    w_inner, w_signal, w_conv, w_memory, factor_in, extra_in, taps_in, gain_in,
    w_turned, w_value_out, w_rim, w_out, aside,
    in_bias, forget_bias, start_scale, factor, extra, taps, gain, sems,
):
    loads = [
        (w_key, w_turned.at[0:64, :]),
        (w_query, w_turned.at[64:128, :]),
        (w_input, w_turned.at[128:136, :]),
        (w_forget, w_turned.at[136:144, :]),
        (w_value, w_value_out),
        (w_inner, w_rim.at[:, 0:128]),
        (w_signal, w_rim.at[:, 128:256]),
        (w_conv, w_out.at[0:128, :]),
        (w_memory, w_out.at[128:256, :]),
        (in_bias_in, in_bias),
        (forget_bias_in, forget_bias),
        (start_scale_in, start_scale),
        (factor_in, factor),
        (extra_in, extra),
        (taps_in, taps),
        (gain_in, gain),
    ]
    loads = [pltpu.make_async_copy(a, b, sems.at[i]) for i, (a, b) in enumerate(loads)]
    for load in loads:
        load.start()
    head = own_tp()
    for load in loads[9:]:
        load.wait()
    w_turned[144:256, :] = jnp.zeros((112, 2048), BF16)
    aside[0:8, :] = rows_of(factor[...].reshape(1, 768))
    aside[8:16, :] = rows_of(extra[pl.ds(head, 1), :])
    aside[16:24, :] = jnp.full((8, 128), in_bias[head], F32)
    aside[24:32, :] = jnp.full((8, 128), forget_bias[head], F32)
    aside[32:40, :] = jnp.full((8, 128), start_scale[head], F32)
    lanes = pl.ds(pl.multiple_of(head * 128, 128), 128)
    gains = gain[...].astype(F32).reshape(1, 1024)
    own_gain = jnp.zeros((1, 128), F32)
    for i in range(8):
        own_gain = jnp.where(head == i, gains[:, 128 * i : 128 * (i + 1)], own_gain)
    aside[40:48, :] = jnp.concatenate(
        [taps[:, lanes].astype(F32), own_gain, jnp.zeros((4, 128), F32)], axis=0
    )
    for load in loads[0:9]:
        load.wait()


def state_body(
    b0, b1, b2, b3, twins, b7, w_turned, w_value, w_rim, aside,
    payload, kqv_out, level_out, rows_out, rows, kqv, level_keep, sems,
):
    head = own_tp()
    blocks = [b0, b1, b2, b3] + [twins.at[pl.ds(96 * i, 96), :] for i in range(3)] + [b7]
    for place, block in zip(places(head), blocks):
        rows[pl.ds(pl.multiple_of(place * 96, 32), 96), :] = block[...]
    savings = [
        pltpu.make_async_copy(rows, rows_out, sems.at[0]),
        pltpu.make_async_copy(kqv, kqv_out, sems.at[1]),
        pltpu.make_async_copy(level_keep, level_out, sems.at[2]),
    ]
    savings[0].start()
    first = dot(rows[...], w_turned[...], ((1,), (1,)))
    values = dot(rows[...], w_value[...]).astype(BF16)
    rim = dot(rows[752:768, :], w_rim[...])
    turned = [jnp.transpose(first[128 * b : 128 * (b + 1), 128:256]) for b in range(6)]
    mine = lax.broadcasted_iota(jnp.int32, (8, 128), 0) == head
    pick = lambda part: jnp.sum(jnp.where(mine, part, 0.0), axis=0, keepdims=True)
    blank = jnp.zeros((2, 128), F32)
    log_input = jnp.concatenate([pick(t[0:8]) for t in turned] + [blank], axis=0) + aside[16:24, :]
    forget = jnp.concatenate([pick(t[8:16]) for t in turned] + [blank], axis=0) + aside[24:32, :]
    log_sig = jnp.minimum(forget, 0.0) - jnp.log1p(jnp.exp(-jnp.abs(forget)))
    log_forget = aside[0:8, :] * log_sig + aside[8:16, :]
    real = lax.broadcasted_iota(jnp.int32, (8, 128), 0) < 6
    until = lax.broadcasted_iota(jnp.int32, (128, 128), 0)
    until = (until <= lax.broadcasted_iota(jnp.int32, (128, 128), 1)).astype(F32)
    cumul = lax.dot_general(
        jnp.where(real, log_forget, 0.0),
        until,
        (((1,), (0,)), ((), ())),
        precision=lax.Precision.HIGHEST,
        preferred_element_type=F32,
    )
    cumul = cumul + row_scan(cumul, jnp.add, 0.0)
    level = jnp.where(real, log_input - cumul, FLOOR)
    total = cumul[5:6, 127:128]
    highest = jnp.max(level, keepdims=True)
    peak = jnp.broadcast_to(total + highest, (1, 128))
    weight = jnp.exp(level - highest)
    columns = jnp.transpose(jnp.concatenate([weight, jnp.zeros((120, 128), F32)], axis=0))
    kqv[:, 0:128] = first[:, 0:128].astype(BF16)
    kqv[:, 128:256] = values
    savings[1].start()
    level_keep[...] = level
    savings[2].start()
    pieces = []
    for b in range(6):
        keys = first[128 * b : 128 * (b + 1), 0:DQK].astype(BF16).astype(F32)
        pieces.append((keys * columns[:, b : b + 1]).astype(BF16))
    state = dot(jnp.concatenate(pieces, axis=0), values, ((0,), (0,)))
    rims = jnp.concatenate([rim[14:16, 0:128], rim[14:16, 128:256]], axis=0)
    sent = packed(state, peak, jnp.broadcast_to(total, (1, 128)), rims)
    for i in range(8):
        payload[i] = sent
    for saving in savings:
        saving.wait()


def local_body(level_in, kqv, local_out, top_out):
    level = level_in[...]
    top = lane_scan(level, jnp.maximum, FLOOR)
    top = jnp.maximum(top, row_scan(top, jnp.maximum, FLOOR))
    tops = jnp.transpose(jnp.concatenate([top, jnp.zeros((120, 128), F32)], axis=0))
    top_out[...] = tops
    row = lax.broadcasted_iota(jnp.int32, (128, 128), 0)
    column = lax.broadcasted_iota(jnp.int32, (128, 128), 1)
    causal = row >= column
    for b in range(6):
        high = 128 * (b + 1)
        query = (kqv[128 * b : high, DQK : 2 * DQK].astype(F32) * DQK**-0.5).astype(BF16)
        scores = dot(query, kqv[0:high, 0:DQK], ((1,), (1,)))
        parts = []
        for u in range(b + 1):
            power = level[u : u + 1, :] - tops[:, b : b + 1]
            if u == b:
                power = jnp.where(causal, power, FLOOR)
            parts.append((scores[:, 128 * u : 128 * (u + 1)] * jnp.exp(power)).astype(BF16))
        weights = parts[0] if b == 0 else jnp.concatenate(parts, axis=1)
        local_out[128 * b : high, :] = dot(weights, kqv[0:high, 128:256]).astype(BF16)


def mixer_body(
    rows_in, w_outer, w_inner, w_signal, w_gate, aside, received, payload, start_state, local_in, tops_in,
    kqv_in, before, gate_out, conv_out, edge_out, first_state, tops, local, query,
    rows, w_all, sems,
):
    loads = [
        pltpu.make_async_copy(w_outer, w_all.at[:, 0:128], sems.at[0]),
        pltpu.make_async_copy(w_inner, w_all.at[:, 128:256], sems.at[1]),
        pltpu.make_async_copy(rows_in, rows, sems.at[2]),
        pltpu.make_async_copy(w_signal, w_all.at[:, 256:384], sems.at[3]),
        pltpu.make_async_copy(w_gate, w_all.at[:, 384:512], sems.at[4]),
        pltpu.make_async_copy(start_state.at[own_tp()], first_state, sems.at[6]),
        pltpu.make_async_copy(tops_in, tops, sems.at[7]),
        pltpu.make_async_copy(local_in, local, sems.at[8]),
        pltpu.make_async_copy(kqv_in.at[:, 0:128], query, sems.at[9]),
    ]
    for load in loads:
        load.start()
    me = own_sp() % 8
    states, peaks, decays, rims = unpack(received)
    earlier = [i < me for i in range(8)]
    state, peak, decay = merged(states, peaks, decays, earlier, earlier)
    rim = jnp.zeros((4, 128), F32)
    for i in range(7):
        rim = jnp.where(me == i + 1, rims[i], rim)
    before[0:64, :] = state
    before[64:72, :] = jnp.concatenate([peak, decay, rim, jnp.zeros((2, 128), F32)], axis=0)
    for load in loads[0:5]:
        load.wait()
    first = dot(rows[...], w_all[:, 0:256])
    second = dot(rows[...], w_all[:, 256:512])
    outer = first[:, 0:128].astype(BF16).astype(F32)
    inner = first[:, 128:256].astype(BF16).astype(F32)
    signal = second[:, 0:128].astype(BF16).astype(F32)
    gate_out[...] = jax.nn.sigmoid(second[:, 128:256].astype(BF16).astype(F32)).astype(BF16)
    tap = aside[40:43, :]
    mixed = inner * signal
    at = lax.broadcasted_iota(jnp.int32, mixed.shape, 0)
    one = jnp.where(at >= 1, pltpu.roll(mixed, 1, 0), 0.0)
    two = jnp.where(at >= 2, pltpu.roll(mixed, 2, 0), 0.0)
    summed = tap[0:1] * two + tap[1:2] * one + tap[2:3] * mixed
    conv_out[...] = (outer * summed).astype(BF16)
    edge_out[0:16, :] = summed[0:16]
    edge_out[16:32, :] = outer[0:16]
    for load in loads[5:]:
        load.wait()


def merged(states, peaks, decays, allowed, upto):
    scales = []
    after = jnp.zeros((1, 128), F32)
    for i in reversed(range(8)):
        scales.append(jnp.where(allowed[i], peaks[i] + after, FLOOR))
        after = after + jnp.where(upto[i], decays[i], 0.0)
    scales = scales[::-1]
    ceiling = functools.reduce(jnp.maximum, scales)
    total = jnp.zeros((DQK, DV), F32)
    for i in range(8):
        factor = jnp.where(allowed[i], jnp.exp(scales[i] - ceiling), 0.0)
        total = total + factor * states[i]
    return total, ceiling, after


def unpack(received):
    wide = [received[(i + 4) % 8].astype(F32) for i in range(8)]
    scales = jnp.concatenate([w[64:65] for w in wide], axis=0)
    scales = scales + pltpu.roll(scales, 127, 1) + pltpu.roll(scales, 126, 1)
    peaks = jnp.broadcast_to(scales[:, 0:1], (8, 128))
    decays = jnp.broadcast_to(scales[:, 3:4], (8, 128))
    return (
        [w[0:64] for w in wide],
        [peaks[i : i + 1] for i in range(8)],
        [decays[i : i + 1] for i in range(8)],
        [w[65:69] for w in wide],
    )


def line_body(received, tops, payload):
    states, peaks, decays, rims = unpack(received)
    every = [True] * 8
    state, peak, decay = merged(states, peaks, decays, every, every)
    sent = packed(state, peak, decay, rims[7])
    for i in range(8):
        payload[i] = sent


def final_body(
    received, aside, before, out_gate, conv, edge, first_state, tops, local, kqv, out
):
    y, z = own_sp() % 8, own_sp() // 8
    states, peaks, decays, rims = unpack(received)
    earlier = [i < z for i in range(8)]
    state, peak, decay = merged(states, peaks, decays, earlier, earlier)
    lifted = aside[32:33, :] + decay
    ceiling = jnp.maximum(lifted, peak)
    state = jnp.exp(lifted - ceiling) * first_state[...] + jnp.exp(peak - ceiling) * state
    lifted = ceiling + before[65:66, :]
    peak = before[64:65, :]
    ceiling = jnp.maximum(lifted, peak)
    state = jnp.exp(lifted - ceiling) * state + jnp.exp(peak - ceiling) * before[0:64, :]
    state = (state * DQK**-0.5).astype(BF16)
    top = tops[...]
    best = jnp.maximum(top, ceiling)
    keep = jnp.exp(top - best)
    bring = jnp.exp(ceiling - best)
    scale = aside[43:44, :]
    for b in range(6):
        here = slice(128 * b, 128 * (b + 1))
        remote = dot(kqv[here, DQK : 2 * DQK], state)
        number = bring[:, b : b + 1] * remote + keep[:, b : b + 1] * local[here, :].astype(F32)
        spread = lax.rsqrt(jnp.mean(number * number, axis=1, keepdims=True) + EPS)
        there = slice(128 * ((b + 3) % 6), 128 * ((b + 3) % 6) + 128)
        out[there, 128:256] = (number * spread * scale * out_gate[here, :].astype(F32)).astype(BF16)
    out[384:768, 0:128] = conv[0:384, :]
    out[0:384, 0:128] = conv[384:768, :]
    rim = before[66:70, :]
    for i in range(7):
        rim = jnp.where(jnp.logical_and(y == 0, z == i + 1), rims[i], rim)
    past = rim[0:2] * rim[2:4]
    tap = aside[40:43, :]
    extra = jnp.concatenate(
        [tap[0:1] * past[0:1] + tap[1:2] * past[1:2], tap[0:1] * past[1:2], jnp.zeros((14, 128), F32)],
        axis=0,
    )
    out[384:400, 0:128] = (edge[16:32, :] * (edge[0:16, :] + extra)).astype(BF16)


def project_body(received, w0, w1, w2, w3, sent, kept, weights, sems):
    tp = own_tp()
    x, core = tp // 2, tp % 2
    loads = []
    for n in range(4):
        for i, weight in enumerate((w0, w2, w3)):
            cut = pl.ds(512 * n, 512)
            loads.append(
                pltpu.make_async_copy(
                    weight.at[:, cut], weights.at[pl.ds(256 * i, 256), cut], sems.at[n, i]
                )
            )
    for load in loads:
        load.start()
    there = pl.ds(pl.multiple_of((1 - core) * 96, 32), 96)
    here = pl.ds(pl.multiple_of(core * 96, 32), 96)
    both = jnp.concatenate(
        [
            jnp.concatenate([received[(x + shift + 2) % 4, rows, :] for shift in (0, 1, 2)], axis=1)
            for rows in (there, here)
        ],
        axis=0,
    )
    low = jnp.concatenate([received[(x + 1) % 4, rows, :] for rows in (there, here)], axis=0)
    for n in range(4):
        for load in loads[3 * n : 3 * n + 3]:
            load.wait()
        cut = slice(512 * n, 512 * (n + 1))
        total = dot(low, w1[:, cut]) + dot(both, weights[:, cut])
        sent[:, cut] = total[0:96].astype(BF16)
        kept[:, cut] = total[96:192]


def add_body(one, other, out):
    out[...] = (one[...] + other[...].astype(F32)).astype(BF16)


def tp_moves(move):
    moves = []
    for i in range(8):
        x, core = move(i // 2, i % 2)
        moves.append((i, (x % 4) * 2 + core))
    return moves


UP = tp_moves(lambda x, c: (x + 1, c))
DOWN = tp_moves(lambda x, c: (x - 1, c))
ACROSS = tp_moves(lambda x, c: (x + 2, c))
SWAP = tp_moves(lambda x, c: (x, 1 - c))
X_GROUPS = [[4, 6, 0, 2], [5, 7, 1, 3]]
TURN = (4, 5, 6, 7, 0, 1, 2, 3)
Y_GROUPS = [[z * 8 + y for y in TURN] for z in range(8)]
Z_GROUPS = [[z * 8 + y for z in TURN] for y in range(8)]


def move(value, pairs):
    return lax.ppermute(value, "tp", pairs)


def to_all(copies, groups):
    return lax.all_to_all(copies, "sp", 0, 0, axis_index_groups=groups)


def on_device(
    tokens, input_norm_gain, w_outer, w_inner, w_signal, taps, w_query, w_key, w_value, w_gate,
    w_input, w_forget, in_bias, forget_bias, factor, extra, start_state, start_scale, head_gain,
    w_conv_out, w_memory_out,
):
    normed = call(
        norm_body,
        [("vmem", (96, 2048), BF16)],
        tag("hbm", tokens, input_norm_gain),
        [
            pltpu.VMEM((96, 2048), BF16),
            pltpu.VMEM((2048,), BF16),
            pltpu.SemaphoreType.DMA((2,)),
        ],
    )
    *prepared, w_out, aside = call(
        prepare_body,
        [
            ("vmem", (256, 2048), BF16),
            ("vmem", (2048, 128), BF16),
            ("vmem", (2048, 256), BF16),
            ("vmem", (256, 2048), BF16),
            ("vmem", (48, 128), F32),
        ],
        tag("vmem", normed)
        + tag("hbm", in_bias, forget_bias, start_scale)
        + tag("hbm", w_key.T, w_query.T, w_input.T, w_forget.T, w_value, w_inner, w_signal)
        + tag("hbm", w_conv_out, w_memory_out, factor, extra.T, taps, head_gain),
        [
            pltpu.SMEM((8,), F32),
            pltpu.SMEM((8,), F32),
            pltpu.SMEM((8,), F32),
            pltpu.VMEM((768,), F32),
            pltpu.VMEM((8, 768), F32),
            pltpu.VMEM((3, 1024), BF16),
            pltpu.VMEM((1024,), BF16),
            pltpu.SemaphoreType.DMA((16,)),
        ],
    )
    low = move(normed, UP)
    far = move(normed, ACROSS)
    high = move(normed, DOWN)
    low, _ = lax.optimization_barrier((low, aside))
    near = call(stack_body, [("vmem", (288, 2048), BF16)], tag("vmem", normed, low, high))
    blocks = [normed, low, high, far, move(near, SWAP), move(far, SWAP)]

    w_sent = w_out
    w_up = move(w_sent, UP)
    w_down = move(w_sent, DOWN)

    payload, kqv, level, rows = call(
        state_body,
        [
            ("vmem", (8, PAYLOAD, 128), BF16),
            ("hbm", (768, 256), BF16),
            ("hbm", (8, 128), F32),
            ("hbm", (768, 2048), BF16),
        ],
        tag("vmem", *blocks, *prepared, aside),
        [
            pltpu.VMEM((768, 2048), BF16),
            pltpu.VMEM((768, 256), BF16),
            pltpu.VMEM((8, 128), F32),
            pltpu.SemaphoreType.DMA((3,)),
        ],
    )
    received = to_all(payload, Y_GROUPS)
    local, tops = call(
        local_body,
        [("load", (768, 128), BF16), ("load", (128, 128), F32)],
        tag("load", level, kqv),
        flops=10**9,
    )
    line = received
    payload = call(
        line_body,
        [("vmem", (8, PAYLOAD, 128), BF16)],
        tag("vmem", line) + tag("hbm", tops),
    )
    w_far = w_out
    w_far = move(w_far, ACROSS)
    received = to_all(payload, Z_GROUPS)
    before, *prefetched = call(
        mixer_body,
        [
            ("vmem", (72, 128), F32),
            ("vmem", (768, 128), BF16),
            ("vmem", (768, 128), BF16),
            ("vmem", (32, 128), F32),
            ("vmem", (64, 128), F32),
            ("vmem", (128, 128), F32),
            ("vmem", (768, 128), BF16),
            ("vmem", (768, 128), BF16),
        ],
        tag("hbm", rows, w_outer, w_inner, w_signal, w_gate)
        + tag("vmem", aside, line)
        + tag("hbm", payload)
        + tag("hbm", start_state, local, tops, kqv),
        [
            pltpu.VMEM((768, 2048), BF16),
            pltpu.VMEM((2048, 512), BF16),
            pltpu.SemaphoreType.DMA((10,)),
        ],
        flops=10**9,
    )
    both = call(
        final_body, [("vmem", (768, 256), BF16)], tag("vmem", received, aside, before, *prefetched)
    )
    mixers = lax.all_to_all(both.reshape(4, 192, 256), "tp", 0, 0, axis_index_groups=X_GROUPS)
    sent, kept = call(
        project_body,
        [("vmem", (96, 2048), BF16), ("vmem", (96, 2048), F32)],
        tag("vmem", mixers) + tag("hbm", w_out) + tag("vmem", w_up) + tag("hbm", w_down, w_far),
        [pltpu.VMEM((768, 2048), BF16), pltpu.SemaphoreType.DMA((4, 3))],
    )
    other = move(sent, SWAP)
    return call(add_body, [("load", (96, 2048), BF16)], tag("vmem", kept, other))


def solution(mesh):
    in_specs = (
        P(("sp", "tp"), None),
        P(),
        P(None, "tp"),
        P(None, "tp"),
        P(None, "tp"),
        P(),
        P(None, "tp"),
        P(None, "tp"),
        P(None, "tp"),
        P(None, "tp"),
        P(),
        P(),
        P(),
        P(),
        P("sp"),
        P("sp", None),
        P(),
        P(),
        P(),
        P("tp", None),
        P("tp", None),
    )

    return jax.shard_map(
        on_device,
        mesh=mesh,
        in_specs=in_specs,
        out_specs=P(("sp", "tp"), None),
        check_vma=False,
    )
```
